256 devices in a mesh: sp: 64 (over z, y, core), tp: 4 (over x).
Axes of the slice: x: 4, y: 4, z: 8, core: 2. Of those that a mesh axis runs over, the one named last changes fastest.
Arguments:
- tokens: bfloat16 [49152, 2048], P('sp'), may hold values from -6 to 6
- input_gain: bfloat16 [2048], replicated, may hold values from 0.099609375 to 1.8984375
- gate_weight: bfloat16 [2048, 2048], P('sp', 'tp'), may hold values from -0.125 to 0.125
- value_weight: bfloat16 [2048, 2048], P('sp', 'tp'), may hold values from -0.125 to 0.125
- inflow_weight: bfloat16 [2048, 4, 128], P('sp', 'tp'), may hold values from -0.125 to 0.125
- readout_weight: bfloat16 [2048, 4, 128], P('sp', 'tp'), may hold values from -0.125 to 0.125
- step_weight: bfloat16 [2048, 2, 32], P('sp', None, 'tp'), may hold values from -0.125 to 0.125
- conv_values: bfloat16 [5, 2048], P(None, 'tp'), may hold values from -2.5 to 2.5
- conv_inflow: bfloat16 [5, 4, 128], P(None, 'tp'), may hold values from -2.5 to 2.5
- conv_readout: bfloat16 [5, 4, 128], P(None, 'tp'), may hold values from -2.5 to 2.5
- log_rate: float32 [2, 49152, 32], P(None, 'sp', 'tp'), may hold values from -20 to 0
- group_gain: bfloat16 [2048], P('tp'), may hold values from 0.099609375 to 1.8984375
- query_weight: bfloat16 [2048, 2048], P('sp', 'tp'), may hold values from -8 to 8
- key_weight: bfloat16 [2048, 512], P('sp', 'tp'), may hold values from -8 to 8
- vector_weight: bfloat16 [2048, 512], P('sp', 'tp'), may hold values from -0.125 to 0.125
- sink_logit: float32 [32], P('tp'), may hold values from 3 to 7
- state_out: bfloat16 [2048, 2048], P('tp', 'sp'), may hold values from -0.125 to 0.125
- window_out: bfloat16 [2048, 2048], P('tp', 'sp'), may hold values from -1 to 1
Outputs:
- mixed: bfloat16 [49152, 2048], P('sp', 'tp')
- log_total: float32 [49152, 32], P('sp', 'tp')
The draws below stay inside these ranges and needn't reach their ends.
All inputs are finite; a program needn't handle non-finite values.
Results may differ from the reference program's by a relative error of at most 0.015.
The reference program's roundings to bfloat16 on the way count: a program that leaves them out, or rounds other values in their place, can miss the bound.
Values may be sent and summed in bfloat16 or wider, within the bound.
No kernel may reach another device: no remote copies, remote signals or barrier semaphores. Data moves between devices by JAX's collectives and lax.ppermute only.
A program may use at most 128 MiB of HBM per device.

```python
import jax
import jax.numpy as jnp
from jax import lax

D = 2048
SSD_HEADS = 32
HEAD_DIM = 64
GROUPS = 4
STATE = 128
CONV = 5
SSD_BLOCK = 128
ATT_HEADS = 32
KV_HEADS = 8
WINDOW = 128
QBLOCK = 256
GRID_W = 64
TOK_DEV = 768
TOKENS = 49152
INNER = 2048
ATT_WIDTH = 2048
KV_WIDTH = 512
N_TP = 4


def shared_query(key):
    base = jax.random.normal(jax.random.fold_in(key, 11), (D, ATT_HEADS, HEAD_DIM), jnp.float32)
    return base * D ** (-0.5)


def draw_query_weight(key, part):
    base = jnp.clip(shared_query(key), -8.0, 8.0)
    return base.reshape(D, ATT_HEADS * HEAD_DIM).astype(jnp.bfloat16)


def draw_key_weight(key, part):
    fresh = jax.random.normal(jax.random.fold_in(key, 12), (D, KV_HEADS, HEAD_DIM), jnp.float32) * D ** (-0.5)
    return jnp.clip(fresh, -8.0, 8.0).reshape(D, KV_HEADS * HEAD_DIM).astype(jnp.bfloat16)


def draw_log_rate(key, part):
    tensor_shape = (2, TOKENS, SSD_HEADS)
    per_group = SSD_HEADS // GROUPS
    chance = 0.5
    ranking = jax.random.permutation(jax.random.fold_in(key, 20), GROUPS)
    quick_group = jax.random.uniform(jax.random.fold_in(key, 21), (GROUPS,), jnp.float32) < chance
    quick_group = jnp.where(ranking == 0, True, jnp.where(ranking == 1, False, quick_group))
    quick_level = jnp.broadcast_to(jnp.repeat(quick_group, per_group)[None, None, :], (2, 1, SSD_HEADS))
    fast_level = jnp.log(jax.random.uniform(jax.random.fold_in(key, 22), (2, 1, SSD_HEADS), jnp.float32, 1.0 / 100.0, 1.0 / 40.0))
    slow_level = jnp.log(jax.random.uniform(jax.random.fold_in(key, 23), (2, 1, SSD_HEADS), jnp.float32, 0.3, 1.5) / TOKENS)
    depth_level = jnp.where(quick_level, fast_level, slow_level)
    blocks = TOKENS // TOK_DEV
    offset_shift = jax.random.uniform(jax.random.fold_in(key, 24), (2, blocks, 1, SSD_HEADS), jnp.float32, -0.7, 0.7)
    offset_shift = jnp.broadcast_to(offset_shift, (2, blocks, TOK_DEV, SSD_HEADS)).reshape(tensor_shape)
    coarse_rough = jax.random.uniform(jax.random.fold_in(key, 25), tensor_shape, jnp.float32, -0.3, 0.3)
    label_marks = jax.random.randint(jax.random.fold_in(key, 26), (1, TOKENS, 1), 0, TOKENS) < 6
    spike_amount = jnp.log(jax.random.uniform(jax.random.fold_in(key, 27), tensor_shape, jnp.float32, 0.3, 1.0))
    final_result = jnp.where(label_marks & jnp.logical_not(quick_level), spike_amount, depth_level + offset_shift + coarse_rough)
    return jnp.clip(final_result, -20.0, 0.0)


def steps_of(own_key, dims, split, least, top_value):
    def one(axis_at, shards_of):
        draws = jax.random.uniform(jax.random.fold_in(jax.random.fold_in(own_key, 6), axis_at), (shards_of,), jnp.float32, least / len(split), top_value / len(split))
        return jnp.repeat(jnp.exp(draws), dims[axis_at] // shards_of).reshape((-1,) + (1,) * (len(dims) - axis_at - 1))

    factor_of = one(*split[0])
    for cut in split[1:]:
        factor_of = factor_of * one(*cut)
    return factor_of


def centred(key, shape, scale, bound, shards=(), kind=jnp.bfloat16):
    factor_of = steps_of(key, shape, shards, -0.22, 0.18) if shards else 1.0
    array = jax.random.normal(key, shape, jnp.float32) * scale * factor_of
    return jnp.minimum(jnp.maximum(array, -bound), bound).astype(kind)


def setup_inputs(seed: int = 0) -> dict:
    key_list = jax.random.split(jax.random.key(seed), 19)
    tokens = centred(key_list[0], (TOKENS, D), 1.0, 6.0, ((0, 64),))
    input_gain = jnp.clip(1.0 + 0.18 * jax.random.normal(key_list[1], (D,), jnp.float32), 0.099609375, 1.8984375).astype(jnp.bfloat16)
    gate_weight = centred(key_list[2], (D, INNER), D ** -0.5, 0.125, ((0, 64), (1, 4)))
    value_weight = centred(key_list[3], (D, INNER), D ** -0.5, 0.125, ((0, 64), (1, 4)))
    inflow_weight = centred(key_list[4], (D, GROUPS, STATE), D ** -0.5, 0.125, ((0, 64), (1, 4)))
    readout_weight = centred(key_list[5], (D, GROUPS, STATE), D ** -0.5, 0.125, ((0, 64), (1, 4)))
    step_weight = centred(key_list[6], (D, 2, SSD_HEADS), D ** -0.5, 0.125, ((0, 64), (2, 4)))
    conv_values = centred(key_list[7], (CONV, INNER), CONV ** -0.5, 2.5, ((1, 4),))
    conv_inflow = centred(key_list[8], (CONV, GROUPS, STATE), CONV ** -0.5, 2.5, ((1, 4),))
    conv_readout = centred(key_list[9], (CONV, GROUPS, STATE), CONV ** -0.5, 2.5, ((1, 4),))
    log_rate = draw_log_rate(jax.random.fold_in(key_list[18], 71), 0)
    group_gain = jnp.clip(1.0 + 0.18 * jax.random.normal(key_list[11], (INNER,), jnp.float32), 0.099609375, 1.8984375).astype(jnp.bfloat16)
    query_weight = draw_query_weight(jax.random.fold_in(key_list[18], 71), 0)
    key_weight = draw_key_weight(jax.random.fold_in(key_list[18], 71), 0)
    vector_weight = centred(key_list[14], (D, KV_WIDTH), D ** -0.5, 0.125, ((0, 64), (1, 4)))
    sink_logit = jnp.clip(3.0 + 4.0 * jax.random.uniform(key_list[15], (ATT_HEADS,), jnp.float32) ** steps_of(key_list[15], (ATT_HEADS,), ((0, 4),), -0.2, 0.2), 3.0, 7.0)
    state_out = centred(key_list[16], (INNER, D), INNER ** -0.5, 0.125, ((0, 4), (1, 64)))
    window_out = centred(key_list[17], (ATT_WIDTH, D), (ATT_WIDTH // 64) ** -0.5, 1.0, ((0, 4), (1, 64)))
    return {"tokens": tokens, "input_gain": input_gain, "gate_weight": gate_weight, "value_weight": value_weight, "inflow_weight": inflow_weight, "readout_weight": readout_weight, "step_weight": step_weight, "conv_values": conv_values, "conv_inflow": conv_inflow, "conv_readout": conv_readout, "log_rate": log_rate, "group_gain": group_gain, "query_weight": query_weight, "key_weight": key_weight, "vector_weight": vector_weight, "sink_logit": sink_logit, "state_out": state_out, "window_out": window_out}


EPS = 1e-06
ROPE_BASE = 10000.0
HIGH = lax.Precision.HIGH

def rope_pairs(part, angle):
    half = part.shape[-1] // 2
    cosine = jnp.cos(angle)[:, None, :]
    sine = jnp.sin(angle)[:, None, :]
    first = part[..., :half]
    second = part[..., half:]
    return jnp.concatenate([first * cosine - second * sine, second * cosine + first * sine], axis=-1)

def axial_rope(heads, positions):
    width = heads.shape[-1]
    quarter = width // 4
    freqs = ROPE_BASE ** (-jnp.arange(quarter).astype(jnp.float32) / quarter)
    row_angle = (positions // GRID_W).astype(jnp.float32)[:, None] * freqs
    col_angle = (positions % GRID_W).astype(jnp.float32)[:, None] * freqs
    half = width // 2
    wide = heads.astype(jnp.float32)
    turned = jnp.concatenate([rope_pairs(wide[..., :half], row_angle), rope_pairs(wide[..., half:], col_angle)], axis=-1)
    return turned.astype(jnp.bfloat16)

def block_ssd(state, inputs):
    xdt, decay, inflow, readout = inputs
    length = decay.shape[0]
    heads = xdt.shape[1]
    groups = inflow.shape[1]
    repeat = heads // groups
    cum = jnp.cumsum(decay, axis=0)
    seg = cum[:, None, :] - cum[None, :, :]
    lower = jnp.arange(length)[:, None] >= jnp.arange(length)[None, :]
    weight = jnp.exp(jnp.where(lower[:, :, None], seg, -jnp.inf))
    intersection = jnp.einsum('lgn,sgn->lsg', readout.astype(jnp.bfloat16), inflow.astype(jnp.bfloat16), preferred_element_type=jnp.float32)
    intersection = jnp.repeat(intersection, repeat, axis=2)
    final_result = jnp.einsum('lsh,shp->lhp', intersection * weight, xdt, precision=HIGH)
    read_heads = jnp.repeat(readout, repeat, axis=1)
    final_result = final_result + jnp.exp(cum)[:, :, None] * jnp.einsum('lhn,hpn->lhp', read_heads, state, precision=HIGH)
    write_heads = jnp.repeat(inflow, repeat, axis=1)
    to_end = jnp.exp(cum[-1][None, :] - cum)
    fresh = jnp.einsum('shp,shn->hpn', xdt * to_end[:, :, None], write_heads, precision=HIGH)
    return (jnp.exp(cum[-1])[:, None, None] * state + fresh, final_result)

def run_blocks(xdt, decay, inflow, readout):
    count = decay.shape[0]
    blocks = count // SSD_BLOCK
    start_state = jnp.zeros((SSD_HEADS, HEAD_DIM, STATE), jnp.float32)
    shaped = (xdt.reshape(blocks, SSD_BLOCK, SSD_HEADS, HEAD_DIM), decay.reshape(blocks, SSD_BLOCK, SSD_HEADS), inflow.reshape(blocks, SSD_BLOCK, GROUPS, STATE), readout.reshape(blocks, SSD_BLOCK, GROUPS, STATE))
    final_state, final_result = lax.scan(block_ssd, start_state, shaped)
    return final_result.reshape(count, SSD_HEADS, HEAD_DIM)

def reference(tokens, input_gain, gate_weight, value_weight, inflow_weight, readout_weight, step_weight, conv_values, conv_inflow, conv_readout, log_rate, group_gain, query_weight, key_weight, vector_weight, sink_logit, state_out, window_out):
    count = tokens.shape[0]
    wide = tokens.astype(jnp.float32)
    normed = (wide * lax.rsqrt(lax.optimization_barrier(jnp.mean(wide * wide, axis=1, keepdims=True)) + EPS) * input_gain.astype(jnp.float32)).astype(jnp.bfloat16)

    def project(weight):
        return jnp.dot(normed, weight.reshape(weight.shape[0], -1), preferred_element_type=jnp.float32)
    gate = project(gate_weight).astype(jnp.bfloat16)
    conv_input = jnp.concatenate([project(value_weight), project(inflow_weight), project(readout_weight)], axis=1).astype(jnp.bfloat16)
    step = jax.nn.softplus(project(step_weight)).reshape(count, 2, SSD_HEADS)
    taps = jnp.concatenate([conv_values, conv_inflow.reshape(CONV, -1), conv_readout.reshape(CONV, -1)], axis=1).astype(jnp.float32)
    reach = CONV // 2
    padded = jnp.pad(conv_input.astype(jnp.float32), ((reach, reach), (0, 0)))
    conv_sum = padded[0:count] * taps[0]
    for tap in range(1, CONV):
        conv_sum = conv_sum + padded[tap:tap + count] * taps[tap]
    conv_out = lax.optimization_barrier(jax.nn.silu(conv_sum).astype(jnp.bfloat16)).astype(jnp.float32)
    xs = conv_out[:, :INNER].reshape(count, SSD_HEADS, HEAD_DIM)
    inflow = conv_out[:, INNER:INNER + GROUPS * STATE].reshape(count, GROUPS, STATE)
    readout = conv_out[:, INNER + GROUPS * STATE:].reshape(count, GROUPS, STATE)
    decay = -jnp.exp(log_rate) * jnp.transpose(step, (1, 0, 2))
    forward = run_blocks(xs * step[:, 0, :, None], decay[0], inflow, readout)
    backward = jnp.flip(run_blocks(jnp.flip(xs * step[:, 1, :, None], 0), jnp.flip(decay[1], 0), jnp.flip(inflow, 0), jnp.flip(readout, 0)), 0)
    combined = (forward + backward).reshape(count, INNER) * jax.nn.silu(gate.astype(jnp.float32))
    grouped = combined.reshape(count, GROUPS, -1)
    grouped = grouped * lax.rsqrt(lax.optimization_barrier(jnp.mean(grouped * grouped, axis=2, keepdims=True)) + EPS)
    state_features = (grouped.reshape(count, INNER) * group_gain.astype(jnp.float32)).astype(jnp.bfloat16)
    repeat = ATT_HEADS // KV_HEADS
    positions = jnp.arange(count, dtype=jnp.int32)
    queries = axial_rope(project(query_weight).astype(jnp.bfloat16).reshape(count, ATT_HEADS, HEAD_DIM), positions)
    keys = axial_rope(project(key_weight).astype(jnp.bfloat16).reshape(count, KV_HEADS, HEAD_DIM), positions)
    vectors = project(vector_weight).astype(jnp.bfloat16).reshape(count, KV_HEADS, HEAD_DIM)
    key_pad = jnp.pad(keys, ((WINDOW, WINDOW), (0, 0), (0, 0)))
    vector_pad = jnp.pad(vectors, ((WINDOW, WINDOW), (0, 0), (0, 0)))
    grouped_q = queries.reshape(count, KV_HEADS, repeat, HEAD_DIM)
    band = QBLOCK + 2 * WINDOW
    sinks = sink_logit.reshape(KV_HEADS, repeat, 1, 1)

    def attend(index):
        start = (index * QBLOCK).astype(jnp.int32)
        block_q = lax.dynamic_slice_in_dim(grouped_q, start, QBLOCK, 0).astype(jnp.float32)
        block_k = lax.dynamic_slice_in_dim(key_pad, start, band, 0).astype(jnp.float32)
        block_v = lax.dynamic_slice_in_dim(vector_pad, start, band, 0).astype(jnp.float32)
        scores = jnp.einsum('qkrd,skd->krqs', block_q, block_k) * HEAD_DIM ** (-0.5)
        query_pos = start + jnp.arange(QBLOCK, dtype=jnp.int32)
        key_pos = start - WINDOW + jnp.arange(band, dtype=jnp.int32)
        valid = (jnp.abs(query_pos[:, None] - key_pos[None, :]) <= WINDOW) & (key_pos >= 0)[None, :] & (key_pos < count)[None, :]
        scores = jnp.where(valid, scores, -jnp.inf)
        top = jnp.maximum(lax.optimization_barrier(jnp.max(scores, axis=-1, keepdims=True)), sinks)
        expo = jnp.exp(scores - top)
        total = lax.optimization_barrier(jnp.sum(expo, axis=-1, keepdims=True)) + jnp.exp(sinks - top)
        probs = lax.optimization_barrier(expo.astype(jnp.bfloat16)).astype(jnp.float32)
        values = jnp.einsum('krqs,skd->qkrd', probs, block_v) / jnp.transpose(total, (2, 0, 1, 3))
        logs = jnp.transpose((top + jnp.log(total))[..., 0], (2, 0, 1)).reshape(QBLOCK, -1)
        return (values.astype(jnp.bfloat16).reshape(QBLOCK, -1), logs)
    feats, logs = lax.map(attend, jnp.arange(count // QBLOCK, dtype=jnp.int32))
    window_features = feats.reshape(count, ATT_WIDTH)
    log_total = logs.reshape(count, ATT_HEADS)
    state_cols = INNER // N_TP
    window_cols = ATT_WIDTH // N_TP
    summed = jnp.zeros((count, D), jnp.float32)
    for group in range(N_TP):
        part = jnp.dot(state_features[:, group * state_cols:(group + 1) * state_cols], state_out[group * state_cols:(group + 1) * state_cols], preferred_element_type=jnp.float32)
        part = part + jnp.dot(window_features[:, group * window_cols:(group + 1) * window_cols], window_out[group * window_cols:(group + 1) * window_cols], preferred_element_type=jnp.float32)
        summed = summed + lax.optimization_barrier(part.astype(jnp.bfloat16)).astype(jnp.float32)
    return (summed.astype(jnp.bfloat16), log_total)
```

```python
import functools

import jax
import jax.numpy as jnp
from jax import lax
from jax.experimental import pallas as pl
from jax.experimental.pallas import tpu as pltpu
from jax.sharding import Mesh
from jax.sharding import PartitionSpec as P

HEAD_DIM = 64
CONV = 5
BLOCK = 128
WINDOW = 128
GRID_W = 64
LANES = 128
SUBLANES = 8
STATE = 128
SP = ("z", "y", "c")
EPS = 1e-06
ROPE_BASE = 10000.0
F32 = jnp.float32
BF16 = jnp.bfloat16


def dot(a, b, dims=((1,), (0,)), precision=None):
    return lax.dot_general(a, b, (dims, ((), ())), precision=precision, preferred_element_type=F32)


def iota(shape, axis):
    return lax.broadcasted_iota(jnp.int32, shape, axis)


def spread(width):
    rows = iota((2 * LANES, width), 0) % LANES
    cols = iota((2 * LANES, width), 1) // HEAD_DIM
    return (rows == cols).astype(BF16)


def two_terms(value):
    high = value.astype(BF16)
    low = (value - high.astype(F32)).astype(BF16)
    return jnp.concatenate([high, low], axis=1)


def front_kernel(raw_ref, taps_ref, rate_ref, spread_ref, conv_ref, cum_ref, dt_ref, fresh_ref, total_ref, end_ref, pad):
    count = conv_ref.shape[0]
    width = conv_ref.shape[1]
    inner = width - 2 * LANES
    blocks = count // BLOCK
    reach = CONV // 2

    def rounded(value):
        return value.astype(BF16).astype(F32)

    pad[pl.ds(8, count), :] = rounded(raw_ref[pl.ds(0, count), pl.ds(0, width)])
    ends = rounded(raw_ref[pl.ds(count, 8), pl.ds(0, width)])
    pad[pl.ds(8 - reach, reach), :] = ends[0:reach]
    pad[pl.ds(8 + count, reach), :] = ends[reach : 2 * reach]
    low = (iota((BLOCK, BLOCK), 0) >= iota((BLOCK, BLOCK), 1)).astype(F32)
    up = (iota((BLOCK, BLOCK), 0) <= iota((BLOCK, BLOCK), 1)).astype(F32)
    heads = inner // HEAD_DIM
    forward = iota((BLOCK, LANES), 1) < heads
    total_ref[...] = jnp.zeros_like(total_ref)
    for block in range(blocks):
        start = block * BLOCK
        acc = pad[pl.ds(start + 8 - reach, BLOCK), :] * taps_ref[0:1, :]
        for tap in range(1, CONV):
            acc = acc + pad[pl.ds(start + 8 - reach + tap, BLOCK), :] * taps_ref[tap : tap + 1, :]
        out = (acc * jax.nn.sigmoid(acc)).astype(BF16)
        conv_ref[pl.ds(start, BLOCK), :] = out
        raw = raw_ref[pl.ds(start, BLOCK), pl.ds(width, LANES)]
        step = jnp.maximum(raw, 0.0) + jnp.log1p(jnp.exp(-jnp.abs(raw)))
        decay = rate_ref[pl.ds(start, BLOCK), :] * step
        cum = jnp.where(
            forward,
            dot(low, decay, precision=lax.Precision.HIGHEST),
            dot(up, decay, precision=lax.Precision.HIGHEST),
        )
        dt_ref[pl.ds(start, BLOCK), :] = step
        cum_ref[pl.ds(start, BLOCK), :] = cum
        total = jnp.where(forward[0:1], cum[BLOCK - 1 : BLOCK], cum[0:1])
        total_ref[block : block + 1, :] = total
        weight = jnp.exp(total - cum) * step
        weight = dot(two_terms(weight), spread_ref[...])
        xs = out[:, 0:inner].astype(F32)
        scaled = (weight * jnp.concatenate([xs, xs], axis=1)).astype(BF16)
        inflow = out[:, inner : inner + LANES]
        fresh_ref[block] = dot(inflow, scaled, dims=((0,), (0,)))
    keep = dot(two_terms(jnp.exp(total_ref[...])), spread_ref[...])
    forward_end = jnp.zeros((LANES, inner), F32)
    backward_end = jnp.zeros((LANES, inner), F32)
    for block in range(blocks):
        forward_end = keep[block : block + 1, 0:inner] * forward_end + fresh_ref[block, :, 0:inner]
        back = blocks - 1 - block
        backward_end = keep[back : back + 1, inner:] * backward_end + fresh_ref[back, :, inner:]
    logs = jnp.sum(total_ref[...], axis=0, keepdims=True)
    logs = dot(two_terms(jnp.broadcast_to(logs, (2 * SUBLANES, LANES))), spread_ref[...])
    high = logs.astype(BF16)
    low_part = (logs - high.astype(F32)).astype(BF16)
    logs = jnp.where(iota(logs.shape, 0) == 0, high.astype(F32), low_part.astype(F32)).astype(BF16)
    end_ref[0, 0:STATE, :] = forward_end.astype(BF16)
    end_ref[1, 0:STATE, :] = backward_end.astype(BF16)
    end_ref[0, pl.ds(STATE, 2 * SUBLANES), :] = logs[:, 0:inner]
    end_ref[1, pl.ds(STATE, 2 * SUBLANES), :] = logs[:, inner:]


def inner_kernel(conv_ref, cum_ref, dt_ref, out_ref):
    count, width = conv_ref.shape
    inner = width - 2 * LANES
    heads = inner // HEAD_DIM
    row = iota((BLOCK, BLOCK), 0)
    col = iota((BLOCK, BLOCK), 1)
    low = row >= col
    even = iota((BLOCK, LANES), 1) < HEAD_DIM

    def body(block, carry):
        at = pl.ds(pl.multiple_of(block * BLOCK, BLOCK), BLOCK)
        inflow = conv_ref[at, pl.ds(inner, LANES)]
        readout = conv_ref[at, pl.ds(inner + LANES, LANES)]
        meet = dot(readout, inflow, dims=((1,), (1,)))
        cum = cum_ref[at, :]
        cum_t = cum.T
        dt_t = dt_ref[at, :].T
        for pair in range(heads // 2):
            mats = []
            for h in (2 * pair, 2 * pair + 1):
                b = heads + h
                gap = jnp.where(low, cum[:, h : h + 1] - cum_t[h : h + 1], cum[:, b : b + 1] - cum_t[b : b + 1])
                ahead = dt_t[h : h + 1]
                behind = dt_t[b : b + 1]
                step = jnp.where(low, ahead + jnp.where(row == col, behind, 0.0), behind)
                mats.append((jnp.exp(gap) * step * meet).astype(BF16))
            xs = conv_ref[at, pl.ds(pair * LANES, LANES)]
            zero = jnp.zeros_like(xs)
            both = jnp.concatenate([jnp.where(even, xs, zero), jnp.where(even, zero, xs)], axis=0)
            out_ref[at, pl.ds(pair * LANES, LANES)] = dot(jnp.concatenate(mats, axis=1), both)
        return carry

    lax.fori_loop(0, count // BLOCK, body, 0)


def attention_kernel(place_ref, sink_ref, proj_ref, before_ref, after_ref, cos_ref, sin_ref, feats_ref, logs_ref, keys, values, scores, probs):
    count = feats_ref.shape[0]
    q_width = feats_ref.shape[1]
    groups = before_ref.shape[1] // 2 // HEAD_DIM
    heads = q_width // HEAD_DIM
    repeat = heads // groups
    long = count + 2 * WINDOW
    band = BLOCK + 2 * WINDOW
    quarter = HEAD_DIM // 4

    def turned(value, cos, sin):
        lane = iota(value.shape, 1) % (2 * quarter)
        other = jnp.where(lane < quarter, pltpu.roll(value, LANES - quarter, 1), pltpu.roll(value, quarter, 1))
        return (value * cos + other * sin).astype(BF16)

    def twice(value):
        wide = value.astype(F32)
        swapped = pltpu.roll(wide, HEAD_DIM, 1)
        first = iota(wide.shape, 1) < HEAD_DIM
        return (
            jnp.where(first, wide, swapped).astype(BF16),
            jnp.where(first, swapped, wide).astype(BF16),
        )

    for start, size, ref, left in (
        (0, WINDOW, before_ref, 0),
        (WINDOW, count, proj_ref, q_width),
        (WINDOW + count, WINDOW, after_ref, 0),
    ):
        at = pl.ds(start, size)
        key = turned(ref[:, pl.ds(left, LANES)].astype(F32), cos_ref[at, :], sin_ref[at, :])
        pair = twice(key)
        vals = twice(ref[:, pl.ds(left + LANES, LANES)])
        for g in range(groups):
            keys[g, at, :] = pair[g]
            values[g, at, :] = vals[g]

    far = place_ref[0]
    whole = place_ref[1]
    row = iota((BLOCK, band), 0)
    col = iota((BLOCK, band), 1)
    near = (col - row >= 0) & (col - row <= 2 * WINDOW)
    even = iota((BLOCK, LANES), 1) < HEAD_DIM
    lane = iota((BLOCK, LANES), 1)

    def body(block, carry):
        start = pl.multiple_of(block * BLOCK, BLOCK)
        at = pl.ds(start, BLOCK)
        here = pl.ds(pl.multiple_of(start + WINDOW, BLOCK), BLOCK)
        cos = cos_ref[here, :]
        sin = sin_ref[here, :]
        position = far + start - WINDOW + col
        valid = near & (position >= 0) & (position < whole)
        logs = jnp.zeros((BLOCK, LANES), F32)
        for g in range(groups):
            stack = []
            for pair in range(repeat // 2):
                tile = proj_ref[at, pl.ds((g * repeat // 2 + pair) * LANES, LANES)].astype(F32)
                query = turned(tile, cos, sin) * jnp.asarray(HEAD_DIM**-0.5, BF16)
                zero = jnp.zeros_like(query)
                stack += [jnp.where(even, query, zero), jnp.where(even, zero, query)]
            window = pl.ds(start, band)
            scores[...] = dot(jnp.concatenate(stack, axis=0), keys[g, window, :], dims=((1,), (1,)))
            shares = []
            for r in range(repeat):
                h = g * repeat + r
                part = pl.ds(r * BLOCK, BLOCK)
                score = jnp.where(valid, scores[part, :], -jnp.inf)
                sink = sink_ref[h]
                top = jnp.maximum(jnp.max(score, axis=1, keepdims=True), sink)
                expo = jnp.exp(score - top)
                total = jnp.sum(expo, axis=1, keepdims=True) + jnp.exp(sink - top)
                probs[part, :] = expo.astype(BF16)
                shares.append(1.0 / total)
                logs = jnp.where(lane == h, top + jnp.log(total), logs)
            mixed = dot(probs[...], values[g, window, :])
            for pair in range(repeat // 2):
                left = mixed[2 * pair * BLOCK : (2 * pair + 1) * BLOCK] * shares[2 * pair]
                right = mixed[(2 * pair + 1) * BLOCK : (2 * pair + 2) * BLOCK] * shares[2 * pair + 1]
                feats_ref[at, pl.ds((g * repeat // 2 + pair) * LANES, LANES)] = jnp.where(even, left, right).astype(BF16)
        logs_ref[at, :] = logs[:, 0:heads]
        return carry

    lax.fori_loop(0, count // BLOCK, body, 0)


def final_kernel(proj_ref, conv_ref, cum_ref, fresh_ref, total_ref, came_ref, near_ref, gain_ref, spread_ref, out_ref, held):
    count, inner = out_ref.shape
    blocks = count // BLOCK
    keep = dot(two_terms(jnp.exp(total_ref[...])), spread_ref[...])
    ahead = came_ref[0]
    behind = came_ref[1]
    for block in range(blocks):
        held[block, :, 0:inner] = ahead.astype(BF16)
        ahead = keep[block : block + 1, 0:inner] * ahead + fresh_ref[block, :, 0:inner]
        back = blocks - 1 - block
        held[back, :, inner:] = behind.astype(BF16)
        behind = keep[back : back + 1, inner:] * behind + fresh_ref[back, :, inner:]
    gate_at = proj_ref.shape[1] - inner

    def body(block, carry):
        at = pl.ds(pl.multiple_of(block * BLOCK, BLOCK), BLOCK)
        read = dot(conv_ref[at, pl.ds(inner + LANES, LANES)], held[block])
        reach = dot(two_terms(jnp.exp(cum_ref[at, :])), spread_ref[...])
        read = read * reach
        y = near_ref[at, :] + read[:, 0:inner] + read[:, inner:]
        gate = proj_ref[at, pl.ds(gate_at, inner)].astype(F32)
        y = y * (gate * jax.nn.sigmoid(gate))
        scale = lax.rsqrt(jnp.mean(y * y, axis=1, keepdims=True) + EPS)
        out_ref[at, :] = (y * scale * gain_ref[...]).astype(BF16)
        return carry

    lax.fori_loop(0, blocks, body, 0)


def call(kernel, out_shape, scratch, flops, *args, scalars=0):
    smem = pl.BlockSpec(memory_space=pltpu.SMEM)
    vmem = pl.BlockSpec(memory_space=pltpu.VMEM)
    moved = sum(a.size * a.dtype.itemsize for a in args)
    return pl.pallas_call(
        kernel,
        out_shape=out_shape,
        in_specs=[smem] * scalars + [vmem] * (len(args) - scalars),
        out_specs=jax.tree.map(lambda _: vmem, out_shape),
        scratch_shapes=scratch,
        cost_estimate=pl.CostEstimate(flops=flops, bytes_accessed=moved, transcendentals=0),
        compiler_params=pltpu.CompilerParams(vmem_limit_bytes=40 * 2**20),
    )(*args)


def shape(dims, kind=F32):
    return jax.ShapeDtypeStruct(dims, kind)


def ring(axis, shift, wraps=True):
    sizes = [lax.axis_size(name) for name in SP]
    at = SP.index(axis)
    pairs = []
    for z in range(sizes[0]):
        for y in range(sizes[1]):
            for c in range(sizes[2]):
                place = [z, y, c]
                target = list(place)
                target[at] = place[at] + (shift if c == 0 else -shift)
                if not wraps and not 0 <= target[at] < sizes[at]:
                    continue
                target[at] %= sizes[at]
                number = lambda p: (p[0] * sizes[1] + p[1]) * sizes[2] + p[2]
                pairs.append((number(place), number(target)))
    return pairs


def opened(payload):
    log = payload[STATE : STATE + 1].astype(F32) + payload[STATE + 1 : STATE + 2].astype(F32)
    return payload[:STATE].astype(F32), log


def closed(state, log):
    high = log.astype(BF16)
    low = (log - high.astype(F32)).astype(BF16)
    rest = jnp.zeros((2 * SUBLANES - 2, state.shape[1]), BF16)
    return jnp.concatenate([state.astype(BF16), high, low, rest], axis=0)


def carried_in(ends):
    core = lax.axis_index("c")
    swap = [(0, 1), (1, 0)]
    sibling = lax.ppermute(ends, "c", swap)
    mine = lax.dynamic_index_in_dim(ends, core, 0, keepdims=False)
    other = lax.dynamic_index_in_dim(sibling, core, 0, keepdims=False)
    state, log = opened(mine)
    beside, log_beside = opened(other)
    chip = closed(state * jnp.exp(log_beside) + beside, log + log_beside)
    length = lax.axis_size("y")
    me = jnp.where(core == 0, lax.axis_index("y"), length - 1 - lax.axis_index("y"))
    got = [opened(lax.ppermute(chip, SP, ring("y", k))) for k in range(1, length)]
    state, log = opened(chip)
    inside = jnp.zeros_like(state)
    reach = jnp.zeros_like(log)
    for k in range(1, length):
        value, span = got[k - 1]
        inside = inside + jnp.where(k <= me, value * jnp.exp(reach), 0.0)
        reach = reach + jnp.where(k <= me, span, 0.0)
    whole = inside * jnp.exp(log) + state
    whole_log = log + reach
    for k in reversed(range(1, length)):
        value, span = got[k - 1]
        whole = jnp.where(k > me, whole * jnp.exp(span) + value, whole)
        whole_log = whole_log + jnp.where(k > me, span, 0.0)
    slab = closed(whole, whole_log)
    outer = jnp.zeros_like(state)
    outer_reach = jnp.zeros_like(log)
    for k in range(1, lax.axis_size("z")):
        value, span = opened(lax.ppermute(slab, SP, ring("z", k, False)))
        outer = outer + value * jnp.exp(outer_reach)
        outer_reach = outer_reach + span
    came = outer * jnp.exp(reach) + inside
    there = lax.ppermute(came.astype(BF16), "c", swap).astype(F32)
    near, near_log = opened(lax.dynamic_index_in_dim(sibling, 1 - core, 0, keepdims=False))
    beyond = there * jnp.exp(near_log) + near
    return jnp.stack([jnp.where(core == 0, came, beyond), jnp.where(core == 0, beyond, came)])


def summed(features, weights):
    length = lax.axis_size("x")
    me = lax.axis_index("x")
    half = features.shape[0] // 2
    width = weights.shape[0] // length

    def term(ahead):
        part = lax.dynamic_slice_in_dim(weights, (me + ahead) % length * width, width, 0)
        return dot(features, part, dims=((1,), (1,)))

    up = [(i, (i + 1) % length) for i in range(length)]
    down = [((i + 1) % length, i) for i in range(length)]
    far = term(2).astype(BF16)
    far_top = lax.ppermute(far[:half], "x", up)
    far_bottom = lax.ppermute(far[half:], "x", down)
    plus = term(1)
    minus = term(3)
    plus_bottom = lax.ppermute(plus[half:].astype(BF16), "x", up)
    minus_top = lax.ppermute(minus[:half].astype(BF16), "x", down)
    own = term(0)
    plus_top = (plus[:half].astype(BF16).astype(F32) + far_top.astype(F32)).astype(BF16)
    minus_bottom = (minus[half:].astype(BF16).astype(F32) + far_bottom.astype(F32)).astype(BF16)
    plus_top = lax.ppermute(plus_top, "x", up)
    minus_bottom = lax.ppermute(minus_bottom, "x", down)
    own = own.astype(BF16).astype(F32)
    top = own[:half] + plus_top.astype(F32) + minus_top.astype(F32)
    bottom = own[half:] + plus_bottom.astype(F32) + minus_bottom.astype(F32)
    return jnp.concatenate([top, bottom], axis=0).astype(BF16)


def rope_tables(positions):
    quarter = HEAD_DIM // 4
    freqs = ROPE_BASE ** (-jnp.arange(quarter).astype(F32) / quarter)
    row = (positions // GRID_W).astype(F32)[:, None] * freqs
    col = (positions % GRID_W).astype(F32)[:, None] * freqs
    cos = jnp.concatenate([jnp.cos(row)] * 2 + [jnp.cos(col)] * 2, axis=1)
    sin = jnp.concatenate([-jnp.sin(row), jnp.sin(row), -jnp.sin(col), jnp.sin(col)], axis=1)
    return jnp.concatenate([cos, cos], axis=1), jnp.concatenate([sin, sin], axis=1)


def shards(
    tokens,
    input_gain,
    gate_weight,
    value_weight,
    inflow_weight,
    readout_weight,
    step_weight,
    conv_values,
    conv_inflow,
    conv_readout,
    log_rate,
    group_gain,
    query_weight,
    key_weight,
    vector_weight,
    sink_logit,
    state_out,
    window_out,
):
    count, features = tokens.shape
    offset = lax.axis_index(SP) * count
    whole = count * lax.axis_size(SP)
    rows = gate_weight.shape[0]
    inner = value_weight.shape[1]
    q_width = query_weight.shape[1]
    kv_width = key_weight.shape[1]
    heads = step_weight.shape[2]
    blocks = count // BLOCK
    reach = CONV // 2

    def up_down(value_up, value_down):
        length = lax.axis_size(SP)
        return (
            lax.ppermute(value_up, SP, [(i, i + 1) for i in range(length - 1)]),
            lax.ppermute(value_down, SP, [(i + 1, i) for i in range(length - 1)]),
        )

    steps = step_weight.reshape(rows, 2 * heads)
    padded = jnp.pad(steps, ((0, 0), (0, LANES - 2 * heads)))
    out_rows = jnp.concatenate([state_out, window_out], axis=0).T
    local = jnp.concatenate(
        [
            value_weight,
            inflow_weight.reshape(rows, -1),
            readout_weight.reshape(rows, -1),
            padded,
            query_weight,
            key_weight,
            vector_weight,
            gate_weight,
            out_rows,
        ],
        axis=1,
    )
    gathered = lax.all_gather(local, SP, axis=0, tiled=True)
    width = inner + 2 * STATE
    first = width + LANES
    second = first + q_width + 2 * kv_width + inner

    head_rows, tail_rows = up_down(tokens[count - reach :], tokens[:reach])
    wide = jnp.concatenate(
        [tokens, head_rows, tail_rows, jnp.zeros((2 * SUBLANES - 2 * reach, features), BF16)], axis=0
    ).astype(F32)
    normed = (
        wide * lax.rsqrt(jnp.mean(wide * wide, axis=1, keepdims=True) + EPS) * input_gain.astype(F32)
    ).astype(BF16)
    taps = jnp.concatenate(
        [conv_values, conv_inflow.reshape(CONV, -1), conv_readout.reshape(CONV, -1)], axis=1
    ).astype(F32)
    taps = jnp.pad(taps, ((0, SUBLANES - CONV), (0, 0)))
    rate = -jnp.exp(jnp.transpose(log_rate, (1, 0, 2)).reshape(count, 2 * heads))
    rate = jnp.pad(rate, ((0, 0), (0, LANES - 2 * heads)))
    cos, sin = rope_tables(offset - WINDOW + jnp.arange(count + 2 * WINDOW, dtype=jnp.int32))
    expand = spread(2 * inner)

    raw = dot(normed, gathered[:, :first])
    conv, cum, step, fresh, total, ends = call(
        front_kernel,
        (
            shape((count, width), BF16),
            shape((count, LANES)),
            shape((count, LANES)),
            shape((blocks, STATE, 2 * inner)),
            shape((SUBLANES, LANES)),
            shape((2, STATE + 2 * SUBLANES, inner), BF16),
        ),
        [pltpu.VMEM((count + 2 * SUBLANES, width), F32)],
        10**9,
        raw,
        taps,
        rate,
        expand,
    )
    came = carried_in(ends)
    proj = dot(normed[:count], gathered[:, first:second]).astype(BF16)
    kv = proj[:, q_width : q_width + 2 * kv_width]
    before, after = up_down(kv[count - WINDOW :], kv[:WINDOW])
    near = call(inner_kernel, shape((count, inner)), [], 2 * 10**9, conv, cum, step)
    band = BLOCK + 2 * WINDOW
    groups = kv_width // HEAD_DIM
    stacked = q_width // HEAD_DIM // groups * BLOCK
    window_features, log_total = call(
        attention_kernel,
        (shape((count, q_width), BF16), shape((count, q_width // HEAD_DIM))),
        [
            pltpu.VMEM((groups, count + 2 * WINDOW, LANES), BF16),
            pltpu.VMEM((groups, count + 2 * WINDOW, LANES), BF16),
            pltpu.VMEM((stacked, band), F32),
            pltpu.VMEM((stacked, band), BF16),
        ],
        5 * 10**9,
        jnp.stack([offset, jnp.int32(whole)]),
        sink_logit,
        proj,
        before,
        after,
        cos,
        sin,
        scalars=2,
    )
    state_features = call(
        final_kernel,
        shape((count, inner), BF16),
        [pltpu.VMEM((blocks, STATE, 2 * inner), BF16)],
        10**9,
        proj,
        conv,
        cum,
        fresh,
        total,
        came,
        near,
        group_gain.astype(F32)[None, :],
        expand,
    )
    mixed = summed(jnp.concatenate([state_features, window_features], axis=1), gathered[:, second:])
    return mixed, log_total


def solution(mesh, sizes=(8, 4, 2)):
    torus = Mesh(mesh.devices.reshape(*sizes, mesh.shape["tp"]), SP + ("x",))
    tp = "x"
    return jax.shard_map(
        shards,
        mesh=torus,
        in_specs=(
            P(SP, None),
            P(),
            P(SP, tp),
            P(SP, tp),
            P(SP, tp, None),
            P(SP, tp, None),
            P(SP, None, tp),
            P(None, tp),
            P(None, tp, None),
            P(None, tp, None),
            P(None, SP, tp),
            P(tp),
            P(SP, tp),
            P(SP, tp),
            P(SP, tp),
            P(tp),
            P(tp, SP),
            P(tp, SP),
        ),
        out_specs=(P(SP, tp), P(SP, tp)),
        check_vma=False,
    )
```

```python
import functools

import jax
import jax.numpy as jnp
from jax import lax
from jax.experimental import pallas as pl
from jax.experimental.pallas import tpu as pltpu
from jax.sharding import Mesh
from jax.sharding import PartitionSpec as P


HEAD_DIM = 64
CONV = 5
BLOCK = 128
WINDOW = 128
GRID_W = 64
LANES = 128
SUBLANES = 8
STATE = 128
LIMIT = 16
SP = ("z", "y", "c")
EPS = 1e-06
ROPE_BASE = 10000.0
F32 = jnp.float32
BF16 = jnp.bfloat16


def dot(a, b, dims=((1,), (0,)), precision=None):
    return lax.dot_general(a, b, (dims, ((), ())), precision=precision, preferred_element_type=F32)


def iota(shape, axis):
    return lax.broadcasted_iota(jnp.int32, shape, axis)


def spread(width):
    rows = iota((2 * LANES, width), 0) % LANES
    cols = iota((2 * LANES, width), 1) // HEAD_DIM
    return (rows == cols).astype(BF16)


def two_terms(value):
    high = value.astype(BF16)
    low = (value - high.astype(F32)).astype(BF16)
    return jnp.concatenate([high, low], axis=1)


def front_kernel(raw_ref, taps_ref, rate_ref, spread_ref, conv_ref, cum_ref, dt_ref, fresh_ref, total_ref, end_ref, pad, flat):
    count = conv_ref.shape[0]
    width = conv_ref.shape[1]
    inner = width - 2 * LANES
    blocks = count // BLOCK
    reach = CONV // 2

    def rounded(value):
        return value.astype(BF16).astype(F32)

    pad[pl.ds(8, count), :] = rounded(raw_ref[pl.ds(0, count), pl.ds(0, width)])
    ends = rounded(raw_ref[pl.ds(count, 8), pl.ds(0, width)])
    pad[pl.ds(8 - reach, reach), :] = ends[0:reach]
    pad[pl.ds(8 + count, reach), :] = ends[reach : 2 * reach]
    low = (iota((BLOCK, BLOCK), 0) >= iota((BLOCK, BLOCK), 1)).astype(F32)
    up = (iota((BLOCK, BLOCK), 0) <= iota((BLOCK, BLOCK), 1)).astype(F32)
    heads = inner // HEAD_DIM
    forward = iota((BLOCK, LANES), 1) < heads
    flat[...] = jnp.full_like(flat, -jnp.inf)
    flat[0 : 2 * heads, :] = rate_ref[...]
    total_ref[...] = jnp.zeros_like(total_ref)
    for block in range(blocks):
        start = block * BLOCK
        acc = pad[pl.ds(start + 8 - reach, BLOCK), :] * taps_ref[0:1, :]
        for tap in range(1, CONV):
            acc = acc + pad[pl.ds(start + 8 - reach + tap, BLOCK), :] * taps_ref[tap : tap + 1, :]
        out = (acc * jax.nn.sigmoid(acc)).astype(BF16)
        conv_ref[pl.ds(start, BLOCK), :] = out
        raw = raw_ref[pl.ds(start, BLOCK), pl.ds(width, LANES)]
        step = jnp.maximum(raw, 0.0) + jnp.log1p(jnp.exp(-jnp.abs(raw)))
        rate = flat[:, pl.ds(start, BLOCK)].T
        decay = -jnp.exp(rate) * step
        cum = jnp.where(
            forward,
            dot(low, decay, precision=lax.Precision.HIGHEST),
            dot(up, decay, precision=lax.Precision.HIGHEST),
        )
        dt_ref[pl.ds(start, BLOCK), :] = step
        cum_ref[pl.ds(start, BLOCK), :] = cum
        total = jnp.where(forward[0:1], cum[BLOCK - 1 : BLOCK], cum[0:1])
        total_ref[block : block + 1, :] = total
        weight = jnp.exp(total - cum) * step
        weight = dot(two_terms(weight), spread_ref[...])
        xs = out[:, 0:inner].astype(F32)
        scaled = (weight * jnp.concatenate([xs, xs], axis=1)).astype(BF16)
        inflow = out[:, inner : inner + LANES]
        fresh_ref[block] = dot(inflow, scaled, dims=((0,), (0,))).astype(BF16)
    keep = dot(two_terms(jnp.exp(total_ref[...])), spread_ref[...])
    forward_end = jnp.zeros((LANES, inner), F32)
    backward_end = jnp.zeros((LANES, inner), F32)
    for block in range(blocks):
        forward_end = keep[block : block + 1, 0:inner] * forward_end + fresh_ref[block, :, 0:inner]
        back = blocks - 1 - block
        backward_end = keep[back : back + 1, inner:] * backward_end + fresh_ref[back, :, inner:]
    logs = jnp.sum(total_ref[...], axis=0, keepdims=True)
    logs = dot(two_terms(jnp.broadcast_to(logs, (2 * SUBLANES, LANES))), spread_ref[...])
    high = logs.astype(BF16)
    low_part = (logs - high.astype(F32)).astype(BF16)
    logs = jnp.where(iota(logs.shape, 0) == 0, high.astype(F32), low_part.astype(F32)).astype(BF16)
    end_ref[0, 0:STATE, :] = forward_end.astype(BF16)
    end_ref[1, 0:STATE, :] = backward_end.astype(BF16)
    end_ref[0, pl.ds(STATE, 2 * SUBLANES), :] = logs[:, 0:inner]
    end_ref[1, pl.ds(STATE, 2 * SUBLANES), :] = logs[:, inner:]


def inner_kernel(conv_ref, cum_ref, dt_ref, out_ref):
    count, width = conv_ref.shape
    inner = width - 2 * LANES
    heads = inner // HEAD_DIM
    row = iota((BLOCK, BLOCK), 0)
    col = iota((BLOCK, BLOCK), 1)
    low = row >= col
    even = iota((BLOCK, LANES), 1) < HEAD_DIM

    def body(block, carry):
        at = pl.ds(pl.multiple_of(block * BLOCK, BLOCK), BLOCK)
        inflow = conv_ref[at, pl.ds(inner, LANES)]
        readout = conv_ref[at, pl.ds(inner + LANES, LANES)]
        meet = dot(readout, inflow, dims=((1,), (1,)))
        cum = cum_ref[at, :]
        cum_t = cum.T
        dt_t = dt_ref[at, :].T
        for pair in range(heads // 2):
            mats = []
            for h in (2 * pair, 2 * pair + 1):
                b = heads + h
                gap = jnp.where(low, cum[:, h : h + 1] - cum_t[h : h + 1], cum[:, b : b + 1] - cum_t[b : b + 1])
                ahead = dt_t[h : h + 1]
                behind = dt_t[b : b + 1]
                step = jnp.where(low, ahead + jnp.where(row == col, behind, 0.0), behind)
                mats.append((jnp.exp(gap) * step * meet).astype(BF16))
            xs = conv_ref[at, pl.ds(pair * LANES, LANES)]
            zero = jnp.zeros_like(xs)
            both = jnp.concatenate([jnp.where(even, xs, zero), jnp.where(even, zero, xs)], axis=0)
            out_ref[at, pl.ds(pair * LANES, LANES)] = dot(jnp.concatenate(mats, axis=1), both)
        return carry

    lax.fori_loop(0, count // BLOCK, body, 0)


def attention_kernel(place_ref, sink_ref, proj_ref, before_ref, after_ref, cos_ref, sin_ref, feats_ref, logs_ref, keys, values, scores, probs):
    count = feats_ref.shape[0]
    q_width = feats_ref.shape[1]
    groups = before_ref.shape[1] // 2 // HEAD_DIM
    heads = q_width // HEAD_DIM
    repeat = heads // groups
    band = BLOCK + 2 * WINDOW
    quarter = HEAD_DIM // 4

    def turned(value, cos, sin):
        lane = iota(value.shape, 1) % (2 * quarter)
        other = jnp.where(lane < quarter, pltpu.roll(value, LANES - quarter, 1), pltpu.roll(value, quarter, 1))
        return (value * cos + other * sin).astype(BF16)

    def twice(value):
        wide = value.astype(F32)
        swapped = pltpu.roll(wide, HEAD_DIM, 1)
        first = iota(wide.shape, 1) < HEAD_DIM
        return (
            jnp.where(first, wide, swapped).astype(BF16),
            jnp.where(first, swapped, wide).astype(BF16),
        )

    for start, size, ref, left in (
        (0, WINDOW, before_ref, 0),
        (WINDOW, count, proj_ref, q_width),
        (WINDOW + count, WINDOW, after_ref, 0),
    ):
        at = pl.ds(start, size)
        key = turned(ref[:, pl.ds(left, LANES)].astype(F32), cos_ref[at, :], sin_ref[at, :])
        pair = twice(key)
        vals = twice(ref[:, pl.ds(left + LANES, LANES)])
        for g in range(groups):
            keys[g, at, :] = pair[g]
            values[g, at, :] = vals[g]

    far = place_ref[4]
    whole = place_ref[5]
    row = iota((BLOCK, band), 0)
    col = iota((BLOCK, band), 1)
    near = (col - row >= 0) & (col - row <= 2 * WINDOW)
    even = iota((BLOCK, LANES), 1) < HEAD_DIM
    lane = iota((BLOCK, LANES), 1)

    def body(block, carry):
        start = pl.multiple_of(block * BLOCK, BLOCK)
        at = pl.ds(start, BLOCK)
        here = pl.ds(pl.multiple_of(start + WINDOW, BLOCK), BLOCK)
        cos = cos_ref[here, :]
        sin = sin_ref[here, :]
        position = far + start - WINDOW + col
        valid = near & (position >= 0) & (position < whole)
        logs = jnp.zeros((BLOCK, LANES), F32)
        for g in range(groups):
            stack = []
            for pair in range(repeat // 2):
                tile = proj_ref[at, pl.ds((g * repeat // 2 + pair) * LANES, LANES)].astype(F32)
                query = turned(tile, cos, sin) * jnp.asarray(HEAD_DIM**-0.5, BF16)
                zero = jnp.zeros_like(query)
                stack += [jnp.where(even, query, zero), jnp.where(even, zero, query)]
            window = pl.ds(start, band)
            scores[...] = dot(jnp.concatenate(stack, axis=0), keys[g, window, :], dims=((1,), (1,)))
            shares = []
            for r in range(repeat):
                h = g * repeat + r
                part = pl.ds(r * BLOCK, BLOCK)
                score = jnp.where(valid, scores[part, :], -jnp.inf)
                sink = sink_ref[h]
                top = jnp.maximum(jnp.max(score, axis=1, keepdims=True), sink)
                expo = jnp.exp(score - top)
                total = jnp.sum(expo, axis=1, keepdims=True) + jnp.exp(sink - top)
                probs[part, :] = expo.astype(BF16)
                shares.append(1.0 / total)
                logs = jnp.where(lane == h, top + jnp.log(total), logs)
            mixed = dot(probs[...], values[g, window, :])
            for pair in range(repeat // 2):
                left = mixed[2 * pair * BLOCK : (2 * pair + 1) * BLOCK] * shares[2 * pair]
                right = mixed[(2 * pair + 1) * BLOCK : (2 * pair + 2) * BLOCK] * shares[2 * pair + 1]
                feats_ref[at, pl.ds((g * repeat // 2 + pair) * LANES, LANES)] = jnp.where(even, left, right).astype(BF16)
        logs_ref[at, :] = logs[:, 0:heads]
        return carry

    lax.fori_loop(0, count // BLOCK, body, 0)


def window_out_kernel(place_ref, feats_ref, whole_ref, out_ref, weight_ref, sem):
    inner = weight_ref.shape[1]
    for copy in fetch(whole_ref, inner, weight_ref, sem):
        copy.wait()
    ahead, _, width = out_ref.shape
    for k in range(ahead):
        rows = pl.ds(pl.multiple_of(lax.rem(place_ref[3] + k, ahead) * width, width), width)
        out_ref[k] = dot(feats_ref[...], weight_ref[rows, :], dims=((1,), (1,)))


def start_states(core, fresh_ref, keep, came_ref, there_ref, sibling_ref, held):
    blocks = held.shape[0]
    inner = held.shape[2] // 2
    near, near_log = opened(sibling_ref[1 - core])
    beyond = there_ref[...].astype(F32) * jnp.exp(near_log) + near
    came = came_ref[...].astype(F32)
    ahead = jnp.where(core == 0, came, beyond)
    behind = jnp.where(core == 0, beyond, came)
    for block in range(blocks):
        held[block, :, 0:inner] = ahead.astype(BF16)
        ahead = keep[block : block + 1, 0:inner] * ahead + fresh_ref[block, :, 0:inner].astype(F32)
        back = blocks - 1 - block
        held[back, :, inner:] = behind.astype(BF16)
        behind = keep[back : back + 1, inner:] * behind + fresh_ref[back, :, inner:].astype(F32)


def final_kernel(half, place_ref, proj_ref, conv_ref, cum_ref, near_ref, gain_ref, spread_ref, share_ref, *refs):
    if half == 0:
        fresh_ref, total_ref, came_ref, there_ref, sibling_ref, whole_ref, held, *outs, feats, weight_ref, sem = refs
    else:
        held, whole_ref, *outs, feats, weight_ref, sem = refs
    copies = fetch(whole_ref, 0, weight_ref, sem)
    if half == 0:
        keep = dot(two_terms(jnp.exp(total_ref[...])), spread_ref[...])
        start_states(place_ref[2], fresh_ref, keep, came_ref, there_ref, sibling_ref, held)
    count, inner = near_ref.shape
    blocks = count // BLOCK // 2
    ahead_count, _, width = share_ref.shape
    gate_at = proj_ref.shape[1] - inner

    def body(step, carry):
        block = step + half * blocks
        at = pl.ds(pl.multiple_of(block * BLOCK, BLOCK), BLOCK)
        read = dot(conv_ref[at, pl.ds(inner + LANES, LANES)], held[block])
        reach = dot(two_terms(jnp.exp(cum_ref[at, :])), spread_ref[...])
        read = read * reach
        y = near_ref[at, :] + read[:, 0:inner] + read[:, inner:]
        gate = proj_ref[at, pl.ds(gate_at, inner)].astype(F32)
        y = y * (gate * jax.nn.sigmoid(gate))
        scale = lax.rsqrt(jnp.mean(y * y, axis=1, keepdims=True) + EPS)
        feats[pl.ds(pl.multiple_of(step * BLOCK, BLOCK), BLOCK), :] = (y * scale * gain_ref[...]).astype(BF16)
        return carry

    lax.fori_loop(0, blocks, body, 0)
    for copy in copies:
        copy.wait()
    for k in range(ahead_count):
        rows = pl.ds(pl.multiple_of(lax.rem(place_ref[3] + k, ahead_count) * width, width), width)
        part = share_ref[k, pl.ds(half * blocks * BLOCK, blocks * BLOCK), :]
        part = part + dot(feats[...], weight_ref[rows, :], dims=((1,), (1,)))
        outs[k][...] = part.astype(BF16)


def add_kernel(one_ref, other_ref, out_ref):
    out_ref[...] = (one_ref[...].astype(F32) + other_ref[...].astype(F32)).astype(BF16)


def sum_kernel(*refs):
    *ins, out_ref = refs
    half = ins[0].shape[0]
    for number in range(2):
        parts = [ref[...].astype(F32) for ref in ins[3 * number : 3 * number + 3]]
        out_ref[pl.ds(number * half, half), :] = (parts[0] + parts[1] + parts[2]).astype(BF16)


def pack_kernel(*refs):
    *ins, out_ref, narrow, sems = refs
    at = 0
    copies = []
    for number, ref in enumerate(ins):
        wide = ref.shape[1]
        target = narrow if wide < LANES else out_ref.at[:, pl.ds(at, wide)]
        copies.append(pltpu.make_async_copy(ref, target, sems.at[number]))
        copies[-1].start()
        at += wide
    for copy in copies:
        copy.wait()
    wide = ins[-1].shape[1]
    if wide < LANES:
        at -= wide
        out_ref[:, pl.ds(at, LANES)] = jnp.zeros((out_ref.shape[0], LANES), BF16)
        out_ref[:, pl.ds(at, wide)] = narrow[...]


def packed(rows, width, narrow, *arrays):
    return pl.pallas_call(
        pack_kernel,
        out_shape=jax.ShapeDtypeStruct((rows, width), BF16),
        in_specs=[pl.BlockSpec(memory_space=pl.ANY)] * len(arrays),
        out_specs=pl.BlockSpec(memory_space=pltpu.VMEM),
        scratch_shapes=[pltpu.VMEM((rows, narrow), BF16), pltpu.SemaphoreType.DMA((len(arrays),))],
        cost_estimate=pl.CostEstimate(flops=10**6, bytes_accessed=rows * width * 4, transcendentals=0),
    )(*arrays)


def stack_kernel(*refs):
    *ins, out_ref = refs
    rows = ins[0].shape[0]
    for number, ref in enumerate(ins):
        out_ref[pl.ds(number * rows, rows), :] = ref[...]


def norm_kernel(tokens_ref, head_ref, tail_ref, gain_ref, out_ref):
    count = tokens_ref.shape[0]
    reach = head_ref.shape[0]

    def normed(value):
        wide = value.astype(F32)
        scale = lax.rsqrt(jnp.mean(wide * wide, axis=1, keepdims=True) + EPS)
        return (wide * scale * gain_ref[...]).astype(BF16)

    def body(block, carry):
        at = pl.ds(pl.multiple_of(block * BLOCK, BLOCK), BLOCK)
        out_ref[at, :] = normed(tokens_ref[at, :])
        return carry

    lax.fori_loop(0, count // BLOCK, body, 0)
    ends = jnp.concatenate([head_ref[...].astype(F32), tail_ref[...].astype(F32)], axis=0)
    ends = normed(jnp.concatenate([ends, jnp.zeros((2 * SUBLANES - 2 * reach, ends.shape[1]), F32)], axis=0))
    out_ref[pl.ds(count, 2 * SUBLANES), :] = ends


def placed(place_ref, refs, sizes, target):
    zs, ys, cs = sizes
    rows = refs[0].shape[0] // zs
    for side in range(2):
        own, up, far_top, far_bottom, down = refs[5 * side : 5 * side + 5]
        core = place_ref[2] if side == 0 else 1 - place_ref[2]
        for j in range(ys):
            for k in range(zs):
                ref, at = ((own, k), (up, k), (far_top if k < zs // 2 else far_bottom, k % (zs // 2)), (down, k))[j]
                z = lax.rem(place_ref[0] + k, zs)
                y = lax.rem(place_ref[1] + j, ys)
                to = pl.multiple_of(((z * ys + y) * cs + core) * rows, rows)
                target[pl.ds(to, rows), :] = ref[pl.ds(at * rows, rows), :]


def project_kernel(sizes, place_ref, normed_ref, *refs):
    *pieces, out_ref, whole = refs
    placed(place_ref, pieces, sizes, whole)
    out_ref[...] = dot(normed_ref[pl.ds(0, out_ref.shape[0]), :], whole[...]).astype(out_ref.dtype)


def fetch(whole_ref, first, target, sems):
    rows, columns = target.shape
    parts = sems.shape[0]
    step = rows // parts
    copies = []
    for part in range(parts):
        at = pl.ds(part * step, step)
        copies.append(pltpu.make_async_copy(whole_ref.at[at, pl.ds(first, columns)], target.at[at, :], sems.at[part]))
        copies[-1].start()
    return copies


def gathered(shard):
    deep = lax.axis_size("z")
    long = lax.axis_size("y")
    parts = [shard]
    for k in range(1, deep):
        parts.append(lax.ppermute(shard, "z", [(i, (i - k) % deep) for i in range(deep)]))
    slab = call(stack_kernel, shape((deep * shard.shape[0], shard.shape[1]), BF16), [], 10**6, *parts)
    before = [(i, (i - 1) % long) for i in range(long)]
    after = [(i, (i + 1) % long) for i in range(long)]
    up = lax.ppermute(slab, "y", before)
    down = lax.ppermute(slab, "y", after)
    half = slab.shape[0] // 2
    far_top = lax.ppermute(up[:half], "y", before)
    far_bottom = lax.ppermute(down[half:], "y", after)
    own = [slab, up, far_top, far_bottom, down]
    swap = [(0, 1), (1, 0)]
    return own + [lax.ppermute(piece, "c", swap) for piece in own], up


def column_call(kernel, out_rows, out_kind, tile, first, tiles, scratch, place, whole_args, pieces):
    smem = pl.BlockSpec(memory_space=pltpu.SMEM)
    specs = [smem] + [pl.BlockSpec(a.shape, lambda i: (0, 0)) for a in whole_args]
    specs += [pl.BlockSpec((p.shape[0], tile), lambda i: (0, first + i)) for p in pieces]
    rows = sum(p.shape[0] for p in pieces)
    flops = 2 * rows * tile * tiles * (whole_args[0].shape[0] if whole_args else 256)
    return pl.pallas_call(
        kernel,
        out_shape=jax.ShapeDtypeStruct((out_rows, tile * tiles), out_kind),
        grid=(tiles,),
        in_specs=specs,
        out_specs=pl.BlockSpec((out_rows, tile), lambda i: (0, i)),
        scratch_shapes=scratch,
        cost_estimate=pl.CostEstimate(flops=flops, bytes_accessed=2 * rows * tile * tiles, transcendentals=0),
        compiler_params=pltpu.CompilerParams(vmem_limit_bytes=LIMIT * 2**20),
    )(place, *whole_args, *pieces)


def call(kernel, out_shape, scratch, flops, *args, scalars=0, limit=LIMIT):
    smem = pl.BlockSpec(memory_space=pltpu.SMEM)
    vmem = pl.BlockSpec(memory_space=pltpu.VMEM)
    moved = sum(a.size * a.dtype.itemsize for a in args)
    return pl.pallas_call(
        kernel,
        out_shape=out_shape,
        in_specs=[smem] * scalars + [vmem] * (len(args) - scalars),
        out_specs=jax.tree.map(lambda _: vmem, out_shape),
        scratch_shapes=scratch,
        cost_estimate=pl.CostEstimate(flops=flops, bytes_accessed=moved, transcendentals=0),
        compiler_params=pltpu.CompilerParams(vmem_limit_bytes=limit * 2**20),
    )(*args)


def shape(dims, kind=F32):
    return jax.ShapeDtypeStruct(dims, kind)


def ring(axis, shift, wraps=True):
    sizes = [lax.axis_size(name) for name in SP]
    at = SP.index(axis)
    pairs = []
    for z in range(sizes[0]):
        for y in range(sizes[1]):
            for c in range(sizes[2]):
                place = [z, y, c]
                target = list(place)
                target[at] = place[at] + (shift if c == 0 else -shift)
                if not wraps and not 0 <= target[at] < sizes[at]:
                    continue
                target[at] %= sizes[at]
                number = lambda p: (p[0] * sizes[1] + p[1]) * sizes[2] + p[2]
                pairs.append((number(place), number(target)))
    return pairs


def opened(payload):
    tail = payload[STATE:].astype(F32)
    return payload[:STATE].astype(F32), tail[0:1] + tail[1:2]


def close(out_ref, state, log):
    high = log.astype(BF16).astype(F32)
    row = iota((2 * SUBLANES, state.shape[1]), 0)
    tail = jnp.where(row == 0, high, jnp.where(row == 1, log - high, 0.0))
    out_ref[0:STATE, :] = state.astype(BF16)
    out_ref[pl.ds(STATE, 2 * SUBLANES), :] = tail.astype(BF16)


def rank(place_ref, at, length):
    return jnp.where(place_ref[2] == 0, place_ref[at], length - 1 - place_ref[at])


def chip_kernel(place_ref, ends_ref, sibling_ref, out_ref):
    core = place_ref[2]
    state, log = opened(ends_ref[core])
    beside, log_beside = opened(sibling_ref[core])
    close(out_ref, state * jnp.exp(log_beside) + beside, log + log_beside)


def slab_kernel(length, place_ref, chip_ref, *refs):
    *got, slab_ref, inside_ref, reach_ref = refs
    me = rank(place_ref, 1, length)
    state, log = opened(chip_ref[...])
    got = [opened(ref[...]) for ref in got]
    inside = jnp.zeros_like(state)
    reach = jnp.zeros_like(log)
    for k, (value, span) in enumerate(got, 1):
        inside = inside + jnp.where(k <= me, value * jnp.exp(reach), 0.0)
        reach = reach + jnp.where(k <= me, span, 0.0)
    whole = inside * jnp.exp(log) + state
    whole_log = log + reach
    for k, (value, span) in reversed(list(enumerate(got, 1))):
        whole = jnp.where(k > me, whole * jnp.exp(span) + value, whole)
        whole_log = whole_log + jnp.where(k > me, span, 0.0)
    close(slab_ref, whole, whole_log)
    inside_ref[...] = inside
    reach_ref[...] = jnp.broadcast_to(reach, reach_ref.shape)


def came_kernel(place_ref, inside_ref, reach_ref, *refs):
    *met, out_ref = refs
    outer = jnp.zeros(out_ref.shape, F32)
    outer_reach = jnp.zeros((1, out_ref.shape[1]), F32)
    for ref in met:
        value, span = opened(ref[...])
        outer = outer + value * jnp.exp(outer_reach)
        outer_reach = outer_reach + span
    out_ref[...] = (outer * jnp.exp(reach_ref[0:1, :]) + inside_ref[...]).astype(BF16)


def carried_in(place, ends):
    swap = [(0, 1), (1, 0)]
    sibling = lax.ppermute(ends, "c", swap)
    payload = shape(ends.shape[1:], BF16)
    state = shape((STATE, ends.shape[2]))
    row = shape((SUBLANES, ends.shape[2]))
    chip = call(chip_kernel, payload, [], 10**6, place, ends, sibling, scalars=1)
    got = []
    length = lax.axis_size("y")
    for k in range(1, length):
        got.append(lax.ppermute(chip, SP, ring("y", k)))
    slab, inside, reach = call(
        functools.partial(slab_kernel, length), (payload, state, row), [], 10**6, place, chip, *got, scalars=1
    )
    met = []
    for k in range(1, lax.axis_size("z")):
        met.append(lax.ppermute(slab, SP, ring("z", k, False)))
    came = call(came_kernel, shape(state.shape, BF16), [], 10**6, place, inside, reach, *met, scalars=1)
    there = lax.ppermute(came, "c", swap)
    return came, there, sibling


def summed(terms):
    length = lax.axis_size("x")
    up = [(i, (i + 1) % length) for i in range(length)]
    down = [((i + 1) % length, i) for i in range(length)]
    own_top, plus_top, far_top, minus_top, own_bottom, plus_bottom, far_bottom, minus_bottom = terms
    kind = shape(own_top.shape, BF16)
    far_top = lax.ppermute(far_top, "x", up)
    far_bottom = lax.ppermute(far_bottom, "x", down)
    plus_bottom = lax.ppermute(plus_bottom, "x", up)
    minus_top = lax.ppermute(minus_top, "x", down)
    plus_top = lax.ppermute(call(add_kernel, kind, [], 10**6, plus_top, far_top, limit=8), "x", up)
    minus_bottom = lax.ppermute(call(add_kernel, kind, [], 10**6, minus_bottom, far_bottom, limit=8), "x", down)
    whole = shape((2 * kind.shape[0], kind.shape[1]), BF16)
    return call(sum_kernel, whole, [], 10**6, own_top, plus_top, minus_top, own_bottom, plus_bottom, minus_bottom, limit=8)


def rope_tables(first, count):
    quarter = HEAD_DIM // 4
    lane = jnp.arange(LANES)
    freqs = ROPE_BASE ** (-(lane % quarter).astype(F32) / quarter)
    row = (first // GRID_W + jnp.arange(count // GRID_W)).astype(F32)[:, None] * freqs
    col = jnp.arange(GRID_W).astype(F32)[:, None] * freqs
    sign = jnp.where(lane % (2 * quarter) < quarter, -1.0, 1.0)
    by_row = (lane % HEAD_DIM < HEAD_DIM // 2)[None, None, :]

    def table(of_row, of_col):
        both = jnp.where(by_row, of_row[:, None, :], of_col[None, :, :])
        return both.reshape(count, LANES)

    return table(jnp.cos(row), jnp.cos(col)), table(jnp.sin(row) * sign, jnp.sin(col) * sign)


def shards(
    tokens,
    input_gain,
    gate_weight,
    value_weight,
    inflow_weight,
    readout_weight,
    step_weight,
    conv_values,
    conv_inflow,
    conv_readout,
    log_rate,
    group_gain,
    query_weight,
    key_weight,
    vector_weight,
    sink_logit,
    state_out,
    window_out,
):
    count, features = tokens.shape
    offset = lax.axis_index(SP) * count
    whole = count * lax.axis_size(SP)
    rows = gate_weight.shape[0]
    inner = value_weight.shape[1]
    q_width = query_weight.shape[1]
    kv_width = key_weight.shape[1]
    heads = step_weight.shape[2]
    blocks = count // BLOCK
    reach = CONV // 2

    def up_down(value_up, value_down):
        length = lax.axis_size(SP)
        return (
            lax.ppermute(value_up, SP, [(i, i + 1) for i in range(length - 1)]),
            lax.ppermute(value_down, SP, [(i + 1, i) for i in range(length - 1)]),
        )

    width = inner + 2 * STATE
    first_width = width + LANES
    proj_width = q_width + 2 * kv_width + inner
    out_rows = state_out.shape[0] + window_out.shape[0]
    pack_one = packed(
        rows,
        first_width,
        2 * heads,
        value_weight,
        inflow_weight.reshape(rows, -1),
        readout_weight.reshape(rows, -1),
        step_weight.reshape(rows, 2 * heads),
    )
    pack_two = packed(
        rows,
        proj_width + out_rows,
        2 * heads,
        state_out.T,
        window_out.T,
        query_weight,
        key_weight,
        vector_weight,
        gate_weight,
    )
    rest = lax.all_gather(pack_two, SP, axis=0, tiled=True)
    pieces_one, _ = gathered(pack_one)
    sizes = tuple(lax.axis_size(name) for name in SP)
    place = jnp.stack(
        [lax.axis_index(name) for name in SP + ("x",)] + [offset, jnp.int32(whole)]
    ).astype(jnp.int32)
    cos, sin = rope_tables(offset - WINDOW, count + 2 * WINDOW)
    tokens, cos, sin, place = lax.optimization_barrier((tokens, cos, sin, place))

    head_rows, tail_rows = up_down(tokens[count - reach :], tokens[:reach])
    normed = call(
        norm_kernel,
        shape((count + 2 * SUBLANES, features), BF16),
        [],
        10**7,
        tokens,
        head_rows,
        tail_rows,
        input_gain.astype(F32)[None, :],
    )
    taps = jnp.concatenate(
        [conv_values, conv_inflow.reshape(CONV, -1), conv_readout.reshape(CONV, -1)], axis=1
    ).astype(F32)
    taps = jnp.pad(taps, ((0, SUBLANES - CONV), (0, 0)))
    expand = spread(2 * inner)

    raw = column_call(
        functools.partial(project_kernel, sizes),
        count + 2 * SUBLANES,
        F32,
        first_width,
        0,
        1,
        [pltpu.VMEM((features, first_width), BF16)],
        place,
        [normed],
        pieces_one,
    )
    conv, cum, step, fresh, total, ends = call(
        front_kernel,
        (
            shape((count, width), BF16),
            shape((count, LANES)),
            shape((count, LANES)),
            shape((blocks, STATE, 2 * inner), BF16),
            shape((SUBLANES, LANES)),
            shape((2, STATE + 2 * SUBLANES, inner), BF16),
        ),
        [pltpu.VMEM((count + 2 * SUBLANES, width), F32), pltpu.VMEM((LANES, count), F32)],
        10**9,
        raw,
        taps,
        jnp.transpose(log_rate, (0, 2, 1)).reshape(2 * heads, count),
        expand,
    )
    came = carried_in(place, ends)
    proj = dot(normed[:count], rest[:, out_rows:]).astype(BF16)
    kv = proj[:, q_width : q_width + 2 * kv_width]
    before, after = up_down(kv[count - WINDOW :], kv[:WINDOW])
    near = call(inner_kernel, shape((count, inner)), [], 2 * 10**9, conv, cum, step)
    band = BLOCK + 2 * WINDOW
    groups = kv_width // HEAD_DIM
    stacked = q_width // HEAD_DIM // groups * BLOCK
    window_features, log_total = call(
        attention_kernel,
        (shape((count, q_width), BF16), shape((count, q_width // HEAD_DIM))),
        [
            pltpu.VMEM((groups, count + 2 * WINDOW, LANES), BF16),
            pltpu.VMEM((groups, count + 2 * WINDOW, LANES), BF16),
            pltpu.VMEM((stacked, band), F32),
            pltpu.VMEM((stacked, band), BF16),
        ],
        5 * 10**9,
        place,
        sink_logit,
        proj,
        before,
        after,
        cos,
        sin,
        scalars=2,
    )
    columns = features // lax.axis_size("x")
    smem = pl.BlockSpec(memory_space=pltpu.SMEM)
    vmem = pl.BlockSpec(memory_space=pltpu.VMEM)

    hbm = pl.BlockSpec(memory_space=pltpu.HBM)
    fetched = [pltpu.VMEM((features, inner), BF16), pltpu.SemaphoreType.DMA((4,))]
    share = pl.pallas_call(
        window_out_kernel,
        out_shape=shape((lax.axis_size("x"), count, columns)),
        in_specs=[smem, vmem, hbm],
        out_specs=vmem,
        scratch_shapes=fetched,
        cost_estimate=pl.CostEstimate(flops=4 * 10**9, bytes_accessed=8 * 10**6, transcendentals=0),
        compiler_params=pltpu.CompilerParams(vmem_limit_bytes=LIMIT * 2**20),
    )(place, window_features, rest)
    common = (proj, conv, cum, near, group_gain.astype(F32)[None, :], expand, share)
    parts = lax.axis_size("x")

    def final(half, *args):
        args = common + args
        outs = [shape((count // 2, columns), BF16)] * parts
        if half == 0:
            outs = [shape((blocks, STATE, 2 * inner), BF16)] + outs
        return pl.pallas_call(
            functools.partial(final_kernel, half),
            out_shape=outs,
            in_specs=[smem] + [vmem] * len(args) + [hbm],
            out_specs=[vmem] * len(outs),
            scratch_shapes=[pltpu.VMEM((count // 2, inner), BF16)] + fetched,
            cost_estimate=pl.CostEstimate(flops=3 * 10**9, bytes_accessed=2 * 10**7, transcendentals=0),
            compiler_params=pltpu.CompilerParams(vmem_limit_bytes=LIMIT * 2**20),
        )(place, *args, rest)

    held, *top = final(0, fresh, total, *came)
    bottom = final(1, held)
    terms = [*top, *bottom]
    mixed = summed(terms)
    return mixed, log_total


def solution(mesh, sizes=(8, 4, 2)):
    torus = Mesh(mesh.devices.reshape(*sizes, mesh.shape["tp"]), SP + ("x",))
    tp = "x"
    return jax.shard_map(
        shards,
        mesh=torus,
        in_specs=(
            P(SP, None),
            P(),
            P(SP, tp),
            P(SP, tp),
            P(SP, tp, None),
            P(SP, tp, None),
            P(SP, None, tp),
            P(None, tp),
            P(None, tp, None),
            P(None, tp, None),
            P(None, SP, tp),
            P(tp),
            P(SP, tp),
            P(SP, tp),
            P(SP, tp),
            P(tp),
            P(tp, SP),
            P(tp, SP),
        ),
        out_specs=(P(SP, tp), P(SP, tp)),
        check_vma=False,
    )
```

```python
import functools

import jax
import jax.numpy as jnp
from jax import lax
from jax.experimental import pallas as pl
from jax.experimental.pallas import tpu as pltpu
from jax.sharding import Mesh
from jax.sharding import PartitionSpec as P


HEAD_DIM = 64
CONV = 5
BLOCK = 128
WINDOW = 128
GRID_W = 64
LANES = 128
SUBLANES = 8
STATE = 128
LIMIT = 16
SP = ("z", "y", "c")
EPS = 1e-06
ROPE_BASE = 10000.0
F32 = jnp.float32
BF16 = jnp.bfloat16


def dot(a, b, dims=((1,), (0,)), precision=None):
    return lax.dot_general(a, b, (dims, ((), ())), precision=precision, preferred_element_type=F32)


def iota(shape, axis):
    return lax.broadcasted_iota(jnp.int32, shape, axis)


def spread(width):
    rows = iota((2 * LANES, width), 0) % LANES
    cols = iota((2 * LANES, width), 1) // HEAD_DIM
    return (rows == cols).astype(BF16)


def two_terms(value):
    high = value.astype(BF16)
    low = (value - high.astype(F32)).astype(BF16)
    return jnp.concatenate([high, low], axis=1)


def front_kernel(raw_ref, taps_ref, rate_ref, spread_ref, conv_ref, cum_ref, dt_ref, fresh_ref, total_ref, end_ref, pad, flat, moving, kept):
    count = conv_ref.shape[0]
    width = conv_ref.shape[1]
    inner = width - 2 * LANES
    blocks = count // BLOCK
    reach = CONV // 2

    def rounded(value):
        return value.astype(BF16).astype(F32)

    pad[pl.ds(8, count), :] = rounded(raw_ref[pl.ds(0, count), pl.ds(0, width)])
    ends = rounded(raw_ref[pl.ds(count, 8), pl.ds(0, width)])
    pad[pl.ds(8 - reach, reach), :] = ends[0:reach]
    pad[pl.ds(8 + count, reach), :] = ends[reach : 2 * reach]
    low = (iota((BLOCK, BLOCK), 0) >= iota((BLOCK, BLOCK), 1)).astype(F32)
    up = (iota((BLOCK, BLOCK), 0) <= iota((BLOCK, BLOCK), 1)).astype(F32)
    heads = inner // HEAD_DIM
    forward = iota((BLOCK, LANES), 1) < heads
    flat[...] = jnp.full_like(flat, -jnp.inf)
    flat[0 : 2 * heads, :] = rate_ref[...]
    total_ref[...] = jnp.zeros_like(total_ref)

    def body(block, carry):
        start = pl.multiple_of(block * BLOCK, BLOCK)
        tall = pad[pl.ds(start, BLOCK + 2 * SUBLANES), :]
        acc = tall[SUBLANES - reach : SUBLANES - reach + BLOCK] * taps_ref[0:1, :]
        for tap in range(1, CONV):
            acc = acc + tall[SUBLANES - reach + tap : SUBLANES - reach + tap + BLOCK] * taps_ref[tap : tap + 1, :]
        out = (acc * jax.nn.sigmoid(acc)).astype(BF16)
        conv_ref[pl.ds(start, BLOCK), :] = out
        raw = raw_ref[pl.ds(start, BLOCK), pl.ds(width, LANES)]
        step = jnp.maximum(raw, 0.0) + jnp.log1p(jnp.exp(-jnp.abs(raw)))
        rate = flat[:, pl.ds(start, BLOCK)].T
        decay = -jnp.exp(rate) * step
        cum = jnp.where(
            forward,
            dot(low, decay, precision=lax.Precision.HIGHEST),
            dot(up, decay, precision=lax.Precision.HIGHEST),
        )
        dt_ref[pl.ds(start, BLOCK), :] = step
        cum_ref[pl.ds(start, BLOCK), :] = cum
        total = jnp.where(forward[0:1], cum[BLOCK - 1 : BLOCK], cum[0:1])
        total_ref[pl.ds(block, 1), :] = total
        weight = jnp.exp(total - cum) * step
        weight = dot(two_terms(weight), spread_ref[...])
        xs = out[:, 0:inner].astype(F32)
        scaled = (weight * jnp.concatenate([xs, xs], axis=1)).astype(BF16)
        inflow = out[:, inner : inner + LANES]
        fresh_ref[block] = dot(inflow, scaled, dims=((0,), (0,))).astype(BF16)
        return carry

    lax.fori_loop(0, blocks, body, 0)
    kept[...] = dot(two_terms(jnp.exp(total_ref[...])), spread_ref[...])
    moving[...] = jnp.zeros_like(moving)

    def advance(block, carry):
        back = blocks - 1 - block
        moving[0] = kept[pl.ds(block, 1), 0:inner] * moving[0] + fresh_ref[block, :, 0:inner].astype(F32)
        moving[1] = kept[pl.ds(back, 1), inner:] * moving[1] + fresh_ref[back, :, inner:].astype(F32)
        return carry

    lax.fori_loop(0, blocks, advance, 0)
    logs = jnp.sum(total_ref[...], axis=0, keepdims=True)
    logs = dot(two_terms(jnp.broadcast_to(logs, (2 * SUBLANES, LANES))), spread_ref[...])
    high = logs.astype(BF16)
    low_part = (logs - high.astype(F32)).astype(BF16)
    logs = jnp.where(iota(logs.shape, 0) == 0, high.astype(F32), low_part.astype(F32)).astype(BF16)
    end_ref[0, 0:STATE, :] = moving[0].astype(BF16)
    end_ref[1, 0:STATE, :] = moving[1].astype(BF16)
    end_ref[0, pl.ds(STATE, 2 * SUBLANES), :] = logs[:, 0:inner]
    end_ref[1, pl.ds(STATE, 2 * SUBLANES), :] = logs[:, inner:]


def inner_kernel(conv_ref, cum_ref, dt_ref, out_ref):
    count, width = conv_ref.shape
    inner = width - 2 * LANES
    heads = inner // HEAD_DIM
    row = iota((BLOCK, BLOCK), 0)
    col = iota((BLOCK, BLOCK), 1)
    low = row >= col
    even = iota((BLOCK, LANES), 1) < HEAD_DIM

    def body(block, carry):
        at = pl.ds(pl.multiple_of(block * BLOCK, BLOCK), BLOCK)
        inflow = conv_ref[at, pl.ds(inner, LANES)]
        readout = conv_ref[at, pl.ds(inner + LANES, LANES)]
        meet = dot(readout, inflow, dims=((1,), (1,)))
        cum = cum_ref[at, :]
        cum_t = cum.T
        dt_t = dt_ref[at, :].T
        for pair in range(heads // 2):
            mats = []
            for h in (2 * pair, 2 * pair + 1):
                b = heads + h
                gap = jnp.where(low, cum[:, h : h + 1] - cum_t[h : h + 1], cum[:, b : b + 1] - cum_t[b : b + 1])
                ahead = dt_t[h : h + 1]
                behind = dt_t[b : b + 1]
                step = jnp.where(low, ahead + jnp.where(row == col, behind, 0.0), behind)
                mats.append((jnp.exp(gap) * step * meet).astype(BF16))
            xs = conv_ref[at, pl.ds(pair * LANES, LANES)]
            zero = jnp.zeros_like(xs)
            both = jnp.concatenate([jnp.where(even, xs, zero), jnp.where(even, zero, xs)], axis=0)
            out_ref[at, pl.ds(pair * LANES, LANES)] = dot(jnp.concatenate(mats, axis=1), both)
        return carry

    lax.fori_loop(0, count // BLOCK, body, 0)


def attention_kernel(place_ref, sink_ref, proj_ref, before_ref, after_ref, cos_ref, sin_ref, feats_ref, logs_ref, keys, values, scores, probs):
    count = feats_ref.shape[0]
    q_width = feats_ref.shape[1]
    groups = before_ref.shape[1] // 2 // HEAD_DIM
    heads = q_width // HEAD_DIM
    repeat = heads // groups
    band = BLOCK + 2 * WINDOW
    quarter = HEAD_DIM // 4

    def turned(value, cos, sin):
        lane = iota(value.shape, 1) % (2 * quarter)
        other = jnp.where(lane < quarter, pltpu.roll(value, LANES - quarter, 1), pltpu.roll(value, quarter, 1))
        return (value * cos + other * sin).astype(BF16)

    def twice(value):
        wide = value.astype(F32)
        swapped = pltpu.roll(wide, HEAD_DIM, 1)
        first = iota(wide.shape, 1) < HEAD_DIM
        return (
            jnp.where(first, wide, swapped).astype(BF16),
            jnp.where(first, swapped, wide).astype(BF16),
        )

    for start, size, ref, left in (
        (0, WINDOW, before_ref, 0),
        (WINDOW, count, proj_ref, q_width),
        (WINDOW + count, WINDOW, after_ref, 0),
    ):
        at = pl.ds(start, size)
        key = turned(ref[:, pl.ds(left, LANES)].astype(F32), cos_ref[at, :], sin_ref[at, :])
        pair = twice(key)
        vals = twice(ref[:, pl.ds(left + LANES, LANES)])
        for g in range(groups):
            keys[g, at, :] = pair[g]
            values[g, at, :] = vals[g]

    far = place_ref[4]
    whole = place_ref[5]
    row = iota((BLOCK, band), 0)
    col = iota((BLOCK, band), 1)
    near = (col - row >= 0) & (col - row <= 2 * WINDOW)
    even = iota((BLOCK, LANES), 1) < HEAD_DIM
    lane = iota((BLOCK, LANES), 1)

    def body(block, carry):
        start = pl.multiple_of(block * BLOCK, BLOCK)
        at = pl.ds(start, BLOCK)
        here = pl.ds(pl.multiple_of(start + WINDOW, BLOCK), BLOCK)
        cos = cos_ref[here, :]
        sin = sin_ref[here, :]
        position = far + start - WINDOW + col
        valid = near & (position >= 0) & (position < whole)

        def group(g, logs):
            stack = []
            for pair in range(repeat // 2):
                tile = proj_ref[at, pl.ds(pl.multiple_of((g * (repeat // 2) + pair) * LANES, LANES), LANES)].astype(F32)
                query = turned(tile, cos, sin) * jnp.asarray(HEAD_DIM**-0.5, BF16)
                zero = jnp.zeros_like(query)
                stack += [jnp.where(even, query, zero), jnp.where(even, zero, query)]
            window = pl.ds(start, band)
            scores[...] = dot(jnp.concatenate(stack, axis=0), keys[g, window, :], dims=((1,), (1,)))
            shares = []
            for r in range(repeat):
                h = g * repeat + r
                part = pl.ds(r * BLOCK, BLOCK)
                score = jnp.where(valid, scores[part, :], -jnp.inf)
                sink = sink_ref[h]
                top = jnp.maximum(jnp.max(score, axis=1, keepdims=True), sink)
                expo = jnp.exp(score - top)
                total = jnp.sum(expo, axis=1, keepdims=True) + jnp.exp(sink - top)
                probs[part, :] = expo.astype(BF16)
                shares.append(1.0 / total)
                logs = jnp.where(lane == h, top + jnp.log(total), logs)
            mixed = dot(probs[...], values[g, window, :])
            for pair in range(repeat // 2):
                left = mixed[2 * pair * BLOCK : (2 * pair + 1) * BLOCK] * shares[2 * pair]
                right = mixed[(2 * pair + 1) * BLOCK : (2 * pair + 2) * BLOCK] * shares[2 * pair + 1]
                out_at = pl.ds(pl.multiple_of((g * (repeat // 2) + pair) * LANES, LANES), LANES)
                feats_ref[at, out_at] = jnp.where(even, left, right).astype(BF16)
            return logs

        logs = lax.fori_loop(0, groups, group, jnp.zeros((BLOCK, LANES), F32))
        logs_ref[at, :] = logs[:, 0:heads]
        return carry

    lax.fori_loop(0, count // BLOCK, body, 0)


def window_out_kernel(place_ref, feats_ref, whole_ref, out_ref, weight_ref, sem):
    inner = weight_ref.shape[1]
    for copy in fetch(whole_ref, inner, weight_ref, sem):
        copy.wait()
    ahead, _, width = out_ref.shape

    def body(k, carry):
        rows = pl.ds(pl.multiple_of(lax.rem(place_ref[3] + k, ahead) * width, width), width)
        out_ref[k] = dot(feats_ref[...], weight_ref[rows, :], dims=((1,), (1,)))
        return carry

    lax.fori_loop(0, ahead, body, 0)


def start_states(core, fresh_ref, keep, came_ref, there_ref, sibling_ref, held, moving, kept):
    blocks = held.shape[0]
    inner = held.shape[2] // 2
    near, near_log = opened(sibling_ref[1 - core])
    beyond = there_ref[...].astype(F32) * jnp.exp(near_log) + near
    came = came_ref[...].astype(F32)
    moving[0] = jnp.where(core == 0, came, beyond)
    moving[1] = jnp.where(core == 0, beyond, came)
    kept[...] = keep

    def body(block, carry):
        back = blocks - 1 - block
        held[block, :, 0:inner] = moving[0].astype(BF16)
        held[back, :, inner:] = moving[1].astype(BF16)
        moving[0] = kept[pl.ds(block, 1), 0:inner] * moving[0] + fresh_ref[block, :, 0:inner].astype(F32)
        moving[1] = kept[pl.ds(back, 1), inner:] * moving[1] + fresh_ref[back, :, inner:].astype(F32)
        return carry

    lax.fori_loop(0, blocks, body, 0)


def final_kernel(half, place_ref, proj_ref, conv_ref, cum_ref, near_ref, gain_ref, spread_ref, share_ref, *refs):
    if half == 0:
        fresh_ref, total_ref, came_ref, there_ref, sibling_ref, whole_ref, held, *outs, feats, weight_ref, sem, moving, kept = refs
    else:
        held, whole_ref, *outs, feats, weight_ref, sem = refs
    copies = fetch(whole_ref, 0, weight_ref, sem)
    if half == 0:
        keep = dot(two_terms(jnp.exp(total_ref[...])), spread_ref[...])
        start_states(place_ref[2], fresh_ref, keep, came_ref, there_ref, sibling_ref, held, moving, kept)
    count, inner = near_ref.shape
    blocks = count // BLOCK // 2
    ahead_count, _, width = share_ref.shape
    gate_at = proj_ref.shape[1] - inner

    def body(step, carry):
        block = step + half * blocks
        at = pl.ds(pl.multiple_of(block * BLOCK, BLOCK), BLOCK)
        read = dot(conv_ref[at, pl.ds(inner + LANES, LANES)], held[block])
        reach = dot(two_terms(jnp.exp(cum_ref[at, :])), spread_ref[...])
        read = read * reach
        y = near_ref[at, :] + read[:, 0:inner] + read[:, inner:]
        gate = proj_ref[at, pl.ds(gate_at, inner)].astype(F32)
        y = y * (gate * jax.nn.sigmoid(gate))
        scale = lax.rsqrt(jnp.mean(y * y, axis=1, keepdims=True) + EPS)
        feats[pl.ds(pl.multiple_of(step * BLOCK, BLOCK), BLOCK), :] = (y * scale * gain_ref[...]).astype(BF16)
        return carry

    lax.fori_loop(0, blocks, body, 0)
    for copy in copies:
        copy.wait()
    for k in range(ahead_count):
        rows = pl.ds(pl.multiple_of(lax.rem(place_ref[3] + k, ahead_count) * width, width), width)
        part = share_ref[k, pl.ds(half * blocks * BLOCK, blocks * BLOCK), :]
        part = part + dot(feats[...], weight_ref[rows, :], dims=((1,), (1,)))
        outs[k][...] = part.astype(BF16)


def add_kernel(one_ref, other_ref, out_ref):
    step = 64

    def body(part, carry):
        at = pl.ds(pl.multiple_of(part * step, step), step)
        out_ref[at, :] = (one_ref[at, :].astype(F32) + other_ref[at, :].astype(F32)).astype(BF16)
        return carry

    lax.fori_loop(0, out_ref.shape[0] // step, body, 0)


def sum_kernel(*refs):
    *ins, out_ref = refs
    half = ins[0].shape[0]
    step = 64
    for number in range(2):

        def body(part, carry, number=number):
            at = pl.ds(pl.multiple_of(part * step, step), step)
            to = pl.ds(pl.multiple_of(number * half + part * step, step), step)
            parts = [ref[at, :].astype(F32) for ref in ins[3 * number : 3 * number + 3]]
            out_ref[to, :] = (parts[0] + parts[1] + parts[2]).astype(BF16)
            return carry

        lax.fori_loop(0, half // step, body, 0)


def pack_kernel(*refs):
    *ins, out_ref, narrow, sems = refs
    at = 0
    copies = []
    for number, ref in enumerate(ins):
        wide = ref.shape[1]
        target = narrow if wide < LANES else out_ref.at[:, pl.ds(at, wide)]
        copies.append(pltpu.make_async_copy(ref, target, sems.at[number]))
        copies[-1].start()
        at += wide
    for copy in copies:
        copy.wait()
    wide = ins[-1].shape[1]
    if wide < LANES:
        at -= wide
        out_ref[:, pl.ds(at, LANES)] = jnp.zeros((out_ref.shape[0], LANES), BF16)
        out_ref[:, pl.ds(at, wide)] = narrow[...]


def packed(rows, width, narrow, *arrays):
    return pl.pallas_call(
        pack_kernel,
        out_shape=jax.ShapeDtypeStruct((rows, width), BF16),
        in_specs=[pl.BlockSpec(memory_space=pl.ANY)] * len(arrays),
        out_specs=pl.BlockSpec(memory_space=pltpu.VMEM),
        scratch_shapes=[pltpu.VMEM((rows, narrow), BF16), pltpu.SemaphoreType.DMA((len(arrays),))],
        cost_estimate=pl.CostEstimate(flops=10**6, bytes_accessed=rows * width * 4, transcendentals=0),
    )(*arrays)


def stack_kernel(*refs):
    *ins, out_ref = refs
    rows = ins[0].shape[0]
    for number, ref in enumerate(ins):
        out_ref[pl.ds(number * rows, rows), :] = ref[...]


def norm_kernel(tokens_ref, head_ref, tail_ref, gain_ref, out_ref):
    count = tokens_ref.shape[0]
    reach = head_ref.shape[0]
    step = BLOCK // 2

    def normed(value):
        wide = value.astype(F32)
        scale = lax.rsqrt(jnp.mean(wide * wide, axis=1, keepdims=True) + EPS)
        return (wide * scale * gain_ref[...]).astype(BF16)

    def body(block, carry):
        at = pl.ds(pl.multiple_of(block * step, step), step)
        out_ref[at, :] = normed(tokens_ref[at, :])
        return carry

    lax.fori_loop(0, count // step, body, 0)
    ends = jnp.concatenate([head_ref[...].astype(F32), tail_ref[...].astype(F32)], axis=0)
    ends = normed(jnp.concatenate([ends, jnp.zeros((2 * SUBLANES - 2 * reach, ends.shape[1]), F32)], axis=0))
    out_ref[pl.ds(count, 2 * SUBLANES), :] = ends


def placed(place_ref, refs, sizes, target):
    zs, ys, cs = sizes
    rows = refs[1].shape[0] // zs
    for side in range(2):
        close_by, far = refs[2 * side : 2 * side + 2]
        own, up, down = (close_by.at[pl.ds(i * zs * rows, zs * rows), :] for i in range(3))
        core = place_ref[2] if side == 0 else 1 - place_ref[2]
        for j, ref in ((0, own), (1, up), (2, far), (3, down)):

            def body(k, carry, j=j, ref=ref, core=core):
                z = lax.rem(place_ref[0] + k, zs)
                y = lax.rem(place_ref[1] + j, ys)
                to = pl.multiple_of(((z * ys + y) * cs + core) * rows, rows)
                target[pl.ds(to, rows), :] = ref[pl.ds(pl.multiple_of(k * rows, rows), rows), :]
                return carry

            lax.fori_loop(0, ref.shape[0] // rows, body, 0)


def project_kernel(sizes, place_ref, normed_ref, *refs):
    *pieces, out_ref, whole = refs
    placed(place_ref, pieces, sizes, whole)
    step = 2 * LANES
    out_ref[...] = jnp.zeros_like(out_ref)

    def body(part, carry):
        at = pl.ds(pl.multiple_of(part * step, step), step)
        out_ref[...] += dot(normed_ref[:, at], whole[at, :])
        return carry

    lax.fori_loop(0, whole.shape[0] // step, body, 0)


def fetch(whole_ref, first, target, sems):
    rows, columns = target.shape
    parts = sems.shape[0]
    step = rows // parts
    copies = []
    for part in range(parts):
        at = pl.ds(part * step, step)
        copies.append(pltpu.make_async_copy(whole_ref.at[at, pl.ds(first, columns)], target.at[at, :], sems.at[part]))
        copies[-1].start()
    return copies


def gathered(shard):
    deep = lax.axis_size("z")
    long = lax.axis_size("y")
    parts = [shard]
    for k in range(1, deep):
        parts.append(lax.ppermute(shard, "z", [(i, (i - k) % deep) for i in range(deep)]))
    slab = call(stack_kernel, shape((deep * shard.shape[0], shard.shape[1]), BF16), [], 10**6, *parts)
    before = [(i, (i - 1) % long) for i in range(long)]
    after = [(i, (i + 1) % long) for i in range(long)]
    up = lax.ppermute(slab, "y", before)
    down = lax.ppermute(slab, "y", after)
    half = slab.shape[0] // 2
    far_top = lax.ppermute(up[:half], "y", before)
    far_bottom = lax.ppermute(down[half:], "y", after)
    swap = [(0, 1), (1, 0)]

    def stacked(*parts):
        rows = sum(part.shape[0] for part in parts)
        return call(stack_kernel, shape((rows, shard.shape[1]), BF16), [], 10**6, *parts)

    close_by = stacked(slab, up, down)
    far = stacked(far_top, far_bottom)
    return [close_by, far] + [lax.ppermute(piece, "c", swap) for piece in (close_by, far)]


def column_call(kernel, out_rows, out_kind, tile, first, tiles, scratch, place, whole_args, pieces):
    smem = pl.BlockSpec(memory_space=pltpu.SMEM)
    specs = [smem] + [pl.BlockSpec(a.shape, lambda i: (0, 0)) for a in whole_args]
    specs += [pl.BlockSpec((p.shape[0], tile), lambda i: (0, first + i)) for p in pieces]
    rows = sum(p.shape[0] for p in pieces)
    flops = 2 * rows * tile * tiles * (whole_args[0].shape[0] if whole_args else 256)
    return pl.pallas_call(
        kernel,
        out_shape=jax.ShapeDtypeStruct((out_rows, tile * tiles), out_kind),
        grid=(tiles,),
        in_specs=specs,
        out_specs=pl.BlockSpec((out_rows, tile), lambda i: (0, i)),
        scratch_shapes=scratch,
        cost_estimate=pl.CostEstimate(flops=flops, bytes_accessed=2 * rows * tile * tiles, transcendentals=0),
        compiler_params=pltpu.CompilerParams(vmem_limit_bytes=LIMIT * 2**20),
    )(place, *whole_args, *pieces)


def call(kernel, out_shape, scratch, flops, *args, scalars=0, limit=LIMIT):
    smem = pl.BlockSpec(memory_space=pltpu.SMEM)
    vmem = pl.BlockSpec(memory_space=pltpu.VMEM)
    moved = sum(a.size * a.dtype.itemsize for a in args)
    return pl.pallas_call(
        kernel,
        out_shape=out_shape,
        in_specs=[smem] * scalars + [vmem] * (len(args) - scalars),
        out_specs=jax.tree.map(lambda _: vmem, out_shape),
        scratch_shapes=scratch,
        cost_estimate=pl.CostEstimate(flops=flops, bytes_accessed=moved, transcendentals=0),
        compiler_params=pltpu.CompilerParams(vmem_limit_bytes=limit * 2**20),
    )(*args)


def shape(dims, kind=F32):
    return jax.ShapeDtypeStruct(dims, kind)


def ring(axis, shift, wraps=True):
    sizes = [lax.axis_size(name) for name in SP]
    at = SP.index(axis)
    pairs = []
    for z in range(sizes[0]):
        for y in range(sizes[1]):
            for c in range(sizes[2]):
                place = [z, y, c]
                target = list(place)
                target[at] = place[at] + (shift if c == 0 else -shift)
                if not wraps and not 0 <= target[at] < sizes[at]:
                    continue
                target[at] %= sizes[at]
                number = lambda p: (p[0] * sizes[1] + p[1]) * sizes[2] + p[2]
                pairs.append((number(place), number(target)))
    return pairs


def opened(payload):
    tail = payload[STATE:].astype(F32)
    return payload[:STATE].astype(F32), tail[0:1] + tail[1:2]


def close(out_ref, state, log):
    high = log.astype(BF16).astype(F32)
    row = iota((2 * SUBLANES, state.shape[1]), 0)
    tail = jnp.where(row == 0, high, jnp.where(row == 1, log - high, 0.0))
    out_ref[0:STATE, :] = state.astype(BF16)
    out_ref[pl.ds(STATE, 2 * SUBLANES), :] = tail.astype(BF16)


def rank(place_ref, at, length):
    return jnp.where(place_ref[2] == 0, place_ref[at], length - 1 - place_ref[at])


def chip_kernel(place_ref, ends_ref, sibling_ref, out_ref):
    core = place_ref[2]
    state, log = opened(ends_ref[core])
    beside, log_beside = opened(sibling_ref[core])
    close(out_ref, state * jnp.exp(log_beside) + beside, log + log_beside)


def slab_kernel(length, place_ref, chip_ref, *refs):
    *got, slab_ref, inside_ref, reach_ref = refs
    me = rank(place_ref, 1, length)
    state, log = opened(chip_ref[...])
    got = [opened(ref[...]) for ref in got]
    inside = jnp.zeros_like(state)
    reach = jnp.zeros_like(log)
    for k, (value, span) in enumerate(got, 1):
        inside = inside + jnp.where(k <= me, value * jnp.exp(reach), 0.0)
        reach = reach + jnp.where(k <= me, span, 0.0)
    whole = inside * jnp.exp(log) + state
    whole_log = log + reach
    for k, (value, span) in reversed(list(enumerate(got, 1))):
        whole = jnp.where(k > me, whole * jnp.exp(span) + value, whole)
        whole_log = whole_log + jnp.where(k > me, span, 0.0)
    close(slab_ref, whole, whole_log)
    inside_ref[...] = inside
    reach_ref[...] = jnp.broadcast_to(reach, reach_ref.shape)


def came_kernel(place_ref, inside_ref, reach_ref, *refs):
    *met, out_ref = refs
    factors = []
    far = jnp.zeros((1, out_ref.shape[1]), F32)
    for ref in met:
        factors.append(jnp.exp(far + reach_ref[0:1, :]))
        tail = ref[pl.ds(STATE, 2 * SUBLANES), :].astype(F32)
        far = far + tail[0:1] + tail[1:2]
    step = 32

    def body(part, carry):
        at = pl.ds(pl.multiple_of(part * step, step), step)
        total = inside_ref[at, :]
        for ref, factor in zip(met, factors):
            total = total + ref[at, :].astype(F32) * factor
        out_ref[at, :] = total.astype(BF16)
        return carry

    lax.fori_loop(0, out_ref.shape[0] // step, body, 0)


def carried_in(place, ends):
    swap = [(0, 1), (1, 0)]
    sibling = lax.ppermute(ends, "c", swap)
    payload = shape(ends.shape[1:], BF16)
    state = shape((STATE, ends.shape[2]))
    row = shape((SUBLANES, ends.shape[2]))
    chip = call(chip_kernel, payload, [], 10**6, place, ends, sibling, scalars=1)
    got = []
    length = lax.axis_size("y")
    for k in range(1, length):
        got.append(lax.ppermute(chip, SP, ring("y", k)))
    slab, inside, reach = call(
        functools.partial(slab_kernel, length), (payload, state, row), [], 10**6, place, chip, *got, scalars=1
    )
    met = []
    for k in range(1, lax.axis_size("z")):
        met.append(lax.ppermute(slab, SP, ring("z", k, False)))
    came = call(came_kernel, shape(state.shape, BF16), [], 10**6, place, inside, reach, *met, scalars=1)
    there = lax.ppermute(came, "c", swap)
    return came, there, sibling


def summed(terms):
    length = lax.axis_size("x")
    up = [(i, (i + 1) % length) for i in range(length)]
    down = [((i + 1) % length, i) for i in range(length)]
    own_top, plus_top, far_top, minus_top, own_bottom, plus_bottom, far_bottom, minus_bottom = terms
    kind = shape(own_top.shape, BF16)
    far_top = lax.ppermute(far_top, "x", up)
    far_bottom = lax.ppermute(far_bottom, "x", down)
    plus_bottom = lax.ppermute(plus_bottom, "x", up)
    minus_top = lax.ppermute(minus_top, "x", down)
    plus_top = lax.ppermute(call(add_kernel, kind, [], 10**6, plus_top, far_top, limit=8), "x", up)
    minus_bottom = lax.ppermute(call(add_kernel, kind, [], 10**6, minus_bottom, far_bottom, limit=8), "x", down)
    whole = shape((2 * kind.shape[0], kind.shape[1]), BF16)
    return call(sum_kernel, whole, [], 10**6, own_top, plus_top, minus_top, own_bottom, plus_bottom, minus_bottom, limit=8)


def rope_tables(first, count):
    quarter = HEAD_DIM // 4
    lane = jnp.arange(LANES)
    freqs = ROPE_BASE ** (-(lane % quarter).astype(F32) / quarter)
    row = (first // GRID_W + jnp.arange(count // GRID_W)).astype(F32)[:, None] * freqs
    col = jnp.arange(GRID_W).astype(F32)[:, None] * freqs
    sign = jnp.where(lane % (2 * quarter) < quarter, -1.0, 1.0)
    by_row = (lane % HEAD_DIM < HEAD_DIM // 2)[None, None, :]

    def table(of_row, of_col):
        both = jnp.where(by_row, of_row[:, None, :], of_col[None, :, :])
        return both.reshape(count, LANES)

    return table(jnp.cos(row), jnp.cos(col)), table(jnp.sin(row) * sign, jnp.sin(col) * sign)


def shards(
    tokens,
    input_gain,
    gate_weight,
    value_weight,
    inflow_weight,
    readout_weight,
    step_weight,
    conv_values,
    conv_inflow,
    conv_readout,
    log_rate,
    group_gain,
    query_weight,
    key_weight,
    vector_weight,
    sink_logit,
    state_out,
    window_out,
):
    count, features = tokens.shape
    offset = lax.axis_index(SP) * count
    whole = count * lax.axis_size(SP)
    rows = gate_weight.shape[0]
    inner = value_weight.shape[1]
    q_width = query_weight.shape[1]
    kv_width = key_weight.shape[1]
    heads = step_weight.shape[2]
    blocks = count // BLOCK
    reach = CONV // 2

    def up_down(value_up, value_down):
        length = lax.axis_size(SP)
        return (
            lax.ppermute(value_up, SP, [(i, i + 1) for i in range(length - 1)]),
            lax.ppermute(value_down, SP, [(i + 1, i) for i in range(length - 1)]),
        )

    width = inner + 2 * STATE
    first_width = width + LANES
    proj_width = q_width + 2 * kv_width + inner
    out_rows = state_out.shape[0] + window_out.shape[0]
    pack_one = packed(
        rows,
        first_width,
        2 * heads,
        value_weight,
        inflow_weight.reshape(rows, -1),
        readout_weight.reshape(rows, -1),
        step_weight.reshape(rows, 2 * heads),
    )
    pack_two = packed(
        rows,
        proj_width + out_rows,
        2 * heads,
        state_out.T,
        window_out.T,
        query_weight,
        key_weight,
        vector_weight,
        gate_weight,
    )
    rest = lax.all_gather(pack_two, SP, axis=0, tiled=True)
    pieces_one = gathered(pack_one)
    sizes = tuple(lax.axis_size(name) for name in SP)
    place = jnp.stack(
        [lax.axis_index(name) for name in SP + ("x",)] + [offset, jnp.int32(whole)]
    ).astype(jnp.int32)
    cos, sin = rope_tables(offset - WINDOW, count + 2 * WINDOW)
    tokens, cos, sin, place = lax.optimization_barrier((tokens, cos, sin, place))

    head_rows, tail_rows = up_down(tokens[count - reach :], tokens[:reach])
    normed = call(
        norm_kernel,
        shape((count + 2 * SUBLANES, features), BF16),
        [],
        10**7,
        tokens,
        head_rows,
        tail_rows,
        input_gain.astype(F32)[None, :],
    )
    taps = jnp.concatenate(
        [conv_values, conv_inflow.reshape(CONV, -1), conv_readout.reshape(CONV, -1)], axis=1
    ).astype(F32)
    taps = jnp.pad(taps, ((0, SUBLANES - CONV), (0, 0)))
    expand = spread(2 * inner)

    raw = column_call(
        functools.partial(project_kernel, sizes),
        count + 2 * SUBLANES,
        F32,
        first_width,
        0,
        1,
        [pltpu.VMEM((features, first_width), BF16)],
        place,
        [normed],
        pieces_one,
    )
    conv, cum, step, fresh, total, ends = call(
        front_kernel,
        (
            shape((count, width), BF16),
            shape((count, LANES)),
            shape((count, LANES)),
            shape((blocks, STATE, 2 * inner), BF16),
            shape((SUBLANES, LANES)),
            shape((2, STATE + 2 * SUBLANES, inner), BF16),
        ),
        [pltpu.VMEM((count + 2 * SUBLANES, width), F32), pltpu.VMEM((LANES, count), F32),
            pltpu.VMEM((2, STATE, inner), F32),
            pltpu.VMEM((SUBLANES, 2 * inner), F32),
        ],
        10**9,
        raw,
        taps,
        jnp.transpose(log_rate, (0, 2, 1)).reshape(2 * heads, count),
        expand,
    )
    came = carried_in(place, ends)
    proj = dot(normed[:count], rest[:, out_rows:]).astype(BF16)
    kv = proj[:, q_width : q_width + 2 * kv_width]
    before, after = up_down(kv[count - WINDOW :], kv[:WINDOW])
    near = call(inner_kernel, shape((count, inner)), [], 2 * 10**9, conv, cum, step)
    band = BLOCK + 2 * WINDOW
    groups = kv_width // HEAD_DIM
    stacked = q_width // HEAD_DIM // groups * BLOCK
    window_features, log_total = call(
        attention_kernel,
        (shape((count, q_width), BF16), shape((count, q_width // HEAD_DIM))),
        [
            pltpu.VMEM((groups, count + 2 * WINDOW, LANES), BF16),
            pltpu.VMEM((groups, count + 2 * WINDOW, LANES), BF16),
            pltpu.VMEM((stacked, band), F32),
            pltpu.VMEM((stacked, band), BF16),
        ],
        5 * 10**9,
        place,
        sink_logit,
        proj,
        before,
        after,
        cos,
        sin,
        scalars=2,
    )
    columns = features // lax.axis_size("x")
    smem = pl.BlockSpec(memory_space=pltpu.SMEM)
    vmem = pl.BlockSpec(memory_space=pltpu.VMEM)

    hbm = pl.BlockSpec(memory_space=pltpu.HBM)
    fetched = [pltpu.VMEM((features, inner), BF16), pltpu.SemaphoreType.DMA((4,))]
    share = pl.pallas_call(
        window_out_kernel,
        out_shape=shape((lax.axis_size("x"), count, columns)),
        in_specs=[smem, vmem, hbm],
        out_specs=vmem,
        scratch_shapes=fetched,
        cost_estimate=pl.CostEstimate(flops=4 * 10**9, bytes_accessed=8 * 10**6, transcendentals=0),
        compiler_params=pltpu.CompilerParams(vmem_limit_bytes=LIMIT * 2**20),
    )(place, window_features, rest)
    common = (proj, conv, cum, near, group_gain.astype(F32)[None, :], expand, share)
    parts = lax.axis_size("x")

    moving = [pltpu.VMEM((2, STATE, inner), F32), pltpu.VMEM((SUBLANES, 2 * inner), F32)]

    def final(half, *args):
        args = common + args
        outs = [shape((count // 2, columns), BF16)] * parts
        if half == 0:
            outs = [shape((blocks, STATE, 2 * inner), BF16)] + outs
        return pl.pallas_call(
            functools.partial(final_kernel, half),
            out_shape=outs,
            in_specs=[smem] + [vmem] * len(args) + [hbm],
            out_specs=[vmem] * len(outs),
            scratch_shapes=[pltpu.VMEM((count // 2, inner), BF16)] + fetched + (moving if half == 0 else []),
            cost_estimate=pl.CostEstimate(flops=3 * 10**9, bytes_accessed=2 * 10**7, transcendentals=0),
            compiler_params=pltpu.CompilerParams(vmem_limit_bytes=LIMIT * 2**20),
        )(place, *args, rest)

    held, *top = final(0, fresh, total, *came)
    bottom = final(1, held)
    terms = [*top, *bottom]
    mixed = summed(terms)
    return mixed, log_total


def solution(mesh, sizes=(8, 4, 2)):
    torus = Mesh(mesh.devices.reshape(*sizes, mesh.shape["tp"]), SP + ("x",))
    tp = "x"
    return jax.shard_map(
        shards,
        mesh=torus,
        in_specs=(
            P(SP, None),
            P(),
            P(SP, tp),
            P(SP, tp),
            P(SP, tp, None),
            P(SP, tp, None),
            P(SP, None, tp),
            P(None, tp),
            P(None, tp, None),
            P(None, tp, None),
            P(None, SP, tp),
            P(tp),
            P(SP, tp),
            P(SP, tp),
            P(SP, tp),
            P(tp),
            P(tp, SP),
            P(tp, SP),
        ),
        out_specs=(P(SP, tp), P(SP, tp)),
        check_vma=False,
    )
```
